32 devices in a mesh: sp: 8 (over z, y), tp: 4 (over x, core).
Axes of the slice: x: 2, y: 2, z: 4, core: 2. Of those that a mesh axis runs over, the one named last changes fastest.
Arguments:
- tokens: bfloat16 [3072, 4096], P(('sp', 'tp')), may hold values from -6 to 6
- norm_gain: float32 [4096], replicated, may hold values from 0.1 to 1.9
- w_query: bfloat16 [4096, 2048], P('sp', 'tp'), may hold values from -0.09375 to 0.09375
- w_key: bfloat16 [4096, 512], P('sp', 'tp'), may hold values from -1.5 to 1.5
- w_value: bfloat16 [4096, 512], P('sp', 'tp'), may hold values from -0.09375 to 0.09375
- w_mem_query: bfloat16 [4096, 1024], P('sp', 'tp'), may hold values from -0.09375 to 0.09375
- w_mem_key: bfloat16 [4096, 1024], P('sp', 'tp'), may hold values from -0.09375 to 0.09375
- w_mem_value: bfloat16 [4096, 1024], P('sp', 'tp'), may hold values from -0.09375 to 0.09375
- w_mem_gate: bfloat16 [4096, 1024], P('sp', 'tp'), may hold values from -0.09375 to 0.09375
- w_gates: bfloat16 [4096, 2, 16], replicated, may hold values from -0.09375 to 0.09375
- sinks: float32 [32], P('tp'), may hold values from 2 to 6
- forget_bias: float32 [16], P('tp'), may hold values from 3 to 13
- forget_shift: float32 [3072, 16], P('sp', 'tp'), may hold values from -1 to 0
- w_out: bfloat16 [3072, 4096], P('sp', 'tp'), may hold values from -0.21650635 to 0.21650635
Outputs:
- mixed: bfloat16 [3072, 4096], P('sp', 'tp')
- log_total: float32 [3072, 32], P('sp', 'tp')
The draws below stay inside these ranges and needn't reach their ends.
All inputs are finite; a program needn't handle non-finite values.
Results may differ from the reference program's by a relative error of at most 0.018.
Values may be sent and summed in bfloat16 or wider, within the bound.
A program may use at most 128 MiB of HBM per device.

```python
import math
import jax
import jax.numpy as jnp
from jax import lax

D = 4096
QH = 32
KVH = 8
CELL_SUBSPACES = 16
HD = 64
WINDOW = 128
BLK = 128
TOK_DEV = 384
ITEM_COUNT = 3072
MIX = 3072


def query_base(key):
    normal_noise = jax.random.normal(jax.random.fold_in(key, 101), (D, QH * HD), jnp.float32)
    return jnp.clip(normal_noise, -6.0, 6.0) * D ** (-0.5)


def draw_w_query(key, part):
    return query_base(key).astype(jnp.bfloat16)


def draw_w_key(key, part):
    normal_noise = jax.random.normal(jax.random.fold_in(key, 102), (D, KVH * HD), jnp.float32)
    own_columns = jnp.clip(normal_noise, -6.0, 6.0) * D ** (-0.5)
    return own_columns.astype(jnp.bfloat16)


def draw_forget_bias(key, part):
    ordering = jax.random.permutation(jax.random.fold_in(key, 201), CELL_SUBSPACES)
    slow_heads = ordering < CELL_SUBSPACES // 2
    jitter = jax.random.uniform(jax.random.fold_in(key, 202), (CELL_SUBSPACES,), jnp.float32, -0.3, 0.3)
    fast_values = jax.random.uniform(jax.random.fold_in(key, 203), (CELL_SUBSPACES,), jnp.float32, 3.4, 4.6)
    slow_values = math.log(4.0 * ITEM_COUNT) + jitter
    return jnp.where(slow_heads, slow_values, fast_values).astype(jnp.float32)


def draw_forget_shift(key, part):
    device_count = ITEM_COUNT // TOK_DEV
    spread = jax.random.uniform(jax.random.fold_in(key, 301), (device_count,), jnp.float32, math.log(0.35), math.log(2.8))
    rates = jnp.exp(spread) * (-0.3 / ITEM_COUNT)
    per_element = jnp.repeat(rates, TOK_DEV, total_repeat_length=ITEM_COUNT)
    place_indices = jax.random.randint(jax.random.fold_in(key, 302), (3, CELL_SUBSPACES), 0, ITEM_COUNT)
    stack_tiers = jax.random.uniform(jax.random.fold_in(key, 303), (3, CELL_SUBSPACES), jnp.float32, 0.22, 0.69)
    element_tally = jnp.arange(ITEM_COUNT)[:, None]
    spurt_bundles = jnp.zeros((ITEM_COUNT, CELL_SUBSPACES), jnp.float32)
    for spurt_tally in range(3):
        spurt_bundles = spurt_bundles + jnp.where(element_tally == place_indices[spurt_tally][None, :], stack_tiers[spurt_tally][None, :], 0.0)
    return (per_element[:, None] - spurt_bundles).astype(jnp.float32)


def draw_w_out(key, part):
    normal_noise = jax.random.normal(jax.random.fold_in(key, 401), (MIX, D), jnp.float32)
    row_scale = jnp.where(jnp.arange(MIX) < QH * HD, 2.0, 1.0)
    return (jnp.clip(normal_noise, -6.0, 6.0) * MIX ** (-0.5) * row_scale[:, None]).astype(jnp.bfloat16)


def block_scale(stream_key, extent, pieces, smallest, high):
    gain = 1.0
    for dim, shards_of in pieces:
        draws = jax.random.uniform(jax.random.fold_in(jax.random.fold_in(stream_key, 6), dim), (shards_of,), jnp.float32, smallest / len(pieces), high / len(pieces))
        gain = gain * jnp.repeat(jnp.exp(draws), extent[dim] // shards_of).reshape((-1,) + (1,) * (len(extent) - 1 - dim))
    return gain


def noise(key, shape, scale, reach, cuts=(), held_as=jnp.bfloat16):
    values = scale * jax.random.normal(key, shape, jnp.float32)
    if cuts:
        values = values * block_scale(key, shape, cuts, -0.22, 0.18)
    return jnp.clip(values, -reach, reach).astype(held_as)


def setup_inputs(seed: int = 0) -> dict:
    key_list = jax.random.split(jax.random.key(seed), 15)
    return {
        "tokens": noise(key_list[0], (ITEM_COUNT, D), 1.0, 6.0, ((0, 32),)),
        "norm_gain": jnp.clip(1.0 + 0.18 * jax.random.normal(key_list[1], (D,), jnp.float32), 0.1, 1.9),
        "w_query": draw_w_query(jax.random.fold_in(key_list[14], 71), 0),
        "w_key": draw_w_key(jax.random.fold_in(key_list[14], 71), 0),
        "w_value": noise(key_list[4], (D, KVH * HD), D ** -0.5, 0.09375, ((0, 8), (1, 4))),
        "w_mem_query": noise(key_list[5], (D, CELL_SUBSPACES * HD), D ** -0.5, 0.09375, ((0, 8), (1, 4))),
        "w_mem_key": noise(key_list[6], (D, CELL_SUBSPACES * HD), D ** -0.5, 0.09375, ((0, 8), (1, 4))),
        "w_mem_value": noise(key_list[7], (D, CELL_SUBSPACES * HD), D ** -0.5, 0.09375, ((0, 8), (1, 4))),
        "w_mem_gate": noise(key_list[8], (D, CELL_SUBSPACES * HD), D ** -0.5, 0.09375, ((0, 8), (1, 4))),
        "w_gates": noise(key_list[9], (D, 2, CELL_SUBSPACES), D ** -0.5, 0.09375),
        "sinks": jnp.clip(2.0 + 4.0 * jax.random.uniform(key_list[10], (QH,), jnp.float32) ** block_scale(key_list[10], (QH,), ((0, 4),), -0.2, 0.2), 2.0, 6.0),
        "forget_bias": draw_forget_bias(jax.random.fold_in(key_list[14], 71), 0),
        "forget_shift": draw_forget_shift(jax.random.fold_in(key_list[14], 71), 0),
        "w_out": draw_w_out(jax.random.fold_in(key_list[14], 71), 0),
    }


EPSILON = 1e-06
MASKED = -1e+30
exact_precision = lax.Precision.HIGHEST

def normalize(tokens, norm_gain):
    values = tokens.astype(jnp.float32)
    rescale = lax.rsqrt(lax.optimization_barrier(jnp.mean(values * values, axis=-1, keepdims=True)) + EPSILON)
    return (values * rescale * norm_gain).astype(jnp.bfloat16)

def advance(carried, key_block, value_block, in_block, cumulative):
    memory_state, normalizer, stabilizer = carried
    block_total = cumulative[:, -1]
    decays = block_total[:, None] - cumulative + in_block
    new_stabilizer = jnp.maximum(block_total + stabilizer, lax.optimization_barrier(jnp.max(decays, axis=-1)))
    weights = jnp.exp(decays - new_stabilizer[:, None])
    rescale = jnp.exp(block_total + stabilizer - new_stabilizer)
    new_state = rescale[:, None, None] * memory_state + jnp.einsum('hsv,hsk->hvk', value_block * weights[:, :, None], key_block, precision=exact_precision)
    new_normalizer = rescale[:, None] * normalizer + jnp.einsum('hs,hsk->hk', weights, key_block, precision=exact_precision)
    return (new_state, new_normalizer, new_stabilizer)

def block_step(carried, block_data):
    memory_state, normalizer, stabilizer = carried
    query_block, key_block, value_block, in_block, forget_block = block_data
    length = in_block.shape[-1]
    cumulative = jnp.cumsum(forget_block, axis=-1)
    causal = lax.broadcasted_iota(jnp.int32, (length, length), 0) >= lax.broadcasted_iota(jnp.int32, (length, length), 1)
    log_weight = jnp.where(causal[None], cumulative[:, :, None] - cumulative[:, None, :] + in_block[:, None, :], MASKED)
    row_level = jnp.maximum(cumulative + stabilizer[:, None], lax.optimization_barrier(jnp.max(log_weight, axis=-1)))
    carried_part = jnp.exp(cumulative + stabilizer[:, None] - row_level)
    affinity = jnp.einsum('htd,hsd->hts', query_block, key_block, precision=exact_precision) * jnp.exp(log_weight - row_level[:, :, None])
    numerator = carried_part[:, :, None] * jnp.einsum('hvk,htk->htv', memory_state, query_block, precision=exact_precision) + jnp.einsum('hts,hsv->htv', affinity, value_block, precision=exact_precision)
    denominator = carried_part * jnp.einsum('hk,htk->ht', normalizer, query_block, precision=exact_precision) + lax.optimization_barrier(jnp.sum(affinity, axis=-1))
    recall = numerator / jnp.maximum(jnp.abs(denominator), jnp.exp(-row_level))[:, :, None]
    return (advance(carried, key_block, value_block, in_block, cumulative), recall)

def reference(tokens, norm_gain, w_query, w_key, w_value, w_mem_query, w_mem_key, w_mem_value, w_mem_gate, w_gates, sinks, forget_bias, forget_shift, w_out):
    normed = normalize(tokens, norm_gain)

    def project(weight):
        return jnp.dot(normed, weight, preferred_element_type=jnp.float32).astype(jnp.bfloat16)
    query = project(w_query)
    key_rows = project(w_key)
    value_rows = project(w_value)
    mem_query = project(w_mem_query)
    mem_key = project(w_mem_key)
    mem_value = project(w_mem_value)
    mem_gate = project(w_mem_gate)
    gate_pre = jnp.dot(normed, w_gates.reshape(D, 2 * CELL_SUBSPACES), preferred_element_type=jnp.float32).reshape(ITEM_COUNT, 2, CELL_SUBSPACES)
    group_size = QH // KVH
    block_count = ITEM_COUNT // WINDOW
    q_blocks = query.reshape(block_count, WINDOW, KVH, group_size, HD)
    zero_rim = jnp.zeros((WINDOW, KVH * HD), jnp.bfloat16)
    padded_keys = jnp.concatenate([zero_rim, key_rows], axis=0).reshape(block_count + 1, WINDOW, KVH, HD)
    padded_values = jnp.concatenate([zero_rim, value_rows], axis=0).reshape(block_count + 1, WINDOW, KVH, HD)
    key_window = jnp.concatenate([padded_keys[:-1], padded_keys[1:]], axis=1)
    value_window = jnp.concatenate([padded_values[:-1], padded_values[1:]], axis=1)
    query_index = lax.broadcasted_iota(jnp.int32, (WINDOW, 2 * WINDOW), 0)
    key_index = lax.broadcasted_iota(jnp.int32, (WINDOW, 2 * WINDOW), 1)
    distance = query_index - key_index + WINDOW
    in_band = (distance >= 0) & (distance < WINDOW)
    sink_logit = sinks.reshape(KVH, group_size, 1, 1)

    def one_block(block_data):
        query_block, key_block, value_block, block_index = block_data
        scores = jnp.einsum('qhgd,khd->hgqk', query_block.astype(jnp.float32), key_block.astype(jnp.float32)) * HD ** (-0.5)
        key_position = block_index * WINDOW - WINDOW + key_index
        allowed = in_band & (key_position >= 0)
        scores = jnp.where(allowed[None, None], scores, MASKED)
        ceiling = jnp.maximum(lax.optimization_barrier(jnp.max(scores, axis=-1, keepdims=True)), sink_logit)
        weights = jnp.exp(scores - ceiling)
        partition = jnp.exp(sink_logit - ceiling) + lax.optimization_barrier(jnp.sum(weights, axis=-1, keepdims=True))
        log_part = (ceiling + jnp.log(partition))[..., 0].transpose(2, 0, 1).reshape(WINDOW, QH)
        probs = (weights / partition).astype(jnp.bfloat16)
        head_out = jnp.einsum('hgqk,khd->qhgd', probs.astype(jnp.float32), value_block.astype(jnp.float32))
        return (head_out.astype(jnp.bfloat16).reshape(WINDOW, QH * HD), log_part)
    attn_blocks, log_blocks = lax.map(one_block, (q_blocks, key_window, value_window, jnp.arange(block_count, dtype=jnp.int32)))
    attn_out = attn_blocks.reshape(ITEM_COUNT, QH * HD)
    log_total = log_blocks.reshape(ITEM_COUNT, QH)
    log_in = gate_pre[:, 0, :] - 0.5 * math.log(ITEM_COUNT)
    log_forget = jax.nn.log_sigmoid(gate_pre[:, 1, :] + forget_bias) + forget_shift
    mem_blocks = ITEM_COUNT // BLK

    def blocks(array):
        return array.astype(jnp.float32).reshape(mem_blocks, BLK, CELL_SUBSPACES, HD).transpose(0, 2, 1, 3)

    def gate_blocks(array):
        return array.reshape(mem_blocks, BLK, CELL_SUBSPACES).transpose(0, 2, 1)
    initial = (jnp.zeros((CELL_SUBSPACES, HD, HD), jnp.float32), jnp.zeros((CELL_SUBSPACES, HD), jnp.float32), jnp.full((CELL_SUBSPACES,), MASKED, jnp.float32))
    inputs = (blocks(mem_query), blocks(mem_key) * HD ** (-0.5), blocks(mem_value), gate_blocks(log_in), gate_blocks(log_forget))
    _, recall = lax.scan(block_step, initial, inputs)
    recall = recall.transpose(0, 2, 1, 3).reshape(ITEM_COUNT, CELL_SUBSPACES * HD)
    mem_out = (recall * jax.nn.sigmoid(mem_gate.astype(jnp.float32))).astype(jnp.bfloat16)
    joined = jnp.concatenate([attn_out, mem_out], axis=1)
    mixed = jnp.dot(joined, w_out, preferred_element_type=jnp.float32).astype(jnp.bfloat16)
    return (mixed, log_total)
```

```python
import functools
import math

import jax
import jax.numpy as jnp
from jax import lax
from jax.experimental import pallas as pl
from jax.experimental.pallas import tpu as pltpu
from jax.sharding import PartitionSpec as P

HD = 64
WINDOW = 128
LANES = 128
EPSILON = 1e-06
MASKED = -1e30
MESH = pl.DeviceIdType.MESH


def begin(copy):
    copy.start()


def drain(copy):
    copy.wait_send()


def dot(left, right, **more):
    return jnp.dot(left, right, preferred_element_type=jnp.float32, **more)


def lanes_of(shape):
    return lax.broadcasted_iota(jnp.int32, shape, len(shape) - 1)


def mixer_kernel(
    sizes,
    tokens, gain, packed, shifts, gate_cols, w_out, sinks, bias,
    mixed, totals,
    T, W, GW, O, ACC, PROJ, NUM, ST, EB, HALO, FS, JS, J, LS, LT, LTF, X,
    own_sems, w_send, w_recv, wy_send, wy_recv, f_send, f_recv,
    tz_send, tz_recv, tx_send, tx_recv, tt_send, tt_recv,
    oz_send, oz_recv, oy_send, oy_recv,
    h_send, h_recv, s_send, s_recv,
    jz_send, jz_recv, l_send, l_recv, jx_send, jx_recv, jt_send, jt_recv,
):
    Z, Y, TP, TC, OC = sizes
    XH = TP // 2
    R, D = tokens.shape
    N = R * TP
    KD, C = packed.shape[1:]
    KO = w_out.shape[0]
    RC, RO = R // TC, KO // OC
    S = Z * Y
    sp, tp = lax.axis_index("sp"), lax.axis_index("tp")
    z, y = sp // Y, sp % Y
    twin = tp + 1 - 2 * (tp % 2)
    can_up, can_down = z < Z - 1, z > 0

    def remote(src, dst, send, recv, to_sp, to_tp):
        return pltpu.make_async_remote_copy(
            src_ref=src, dst_ref=dst, send_sem=send, recv_sem=recv,
            device_id={"sp": to_sp, "tp": to_tp}, device_id_type=MESH,
        )

    def side_tp(k):
        return (tp + 2 * k) % TP

    def from_tp(k):
        return (tp + TP - 2 * k) % TP

    def up_z(k):
        return (z + k) % Z

    def back_z(k):
        return (z + Z - k) % Z

    def up_y(k):
        return (y + k) % Y

    def back_y(k):
        return (y + Y - k) % Y

    def w_rows(zz, yy):
        return W.at[pl.ds(pl.multiple_of((zz * Y + yy) * KD, KD), KD), :]

    def w_across(k, source):
        return remote(
            packed.at[up_z(k)], w_rows(source, y), w_send.at[k], w_recv.at[k], up_z(k) * Y + y, tp
        )

    def w_side(k, j, source):
        zz = back_z(k)
        src = packed.at[z] if k == 0 else w_rows(zz, y)
        return remote(
            src, w_rows(zz, source), wy_send.at[k, j - 1], wy_recv.at[k, j - 1], z * Y + up_y(j), tp
        )

    def f_across(k, source):
        return remote(
            shifts.at[up_z(k)], FS.at[source], f_send.at[k], f_recv.at[k], up_z(k) * Y + y, tp
        )

    def t_rows(zz, tt, c):
        start = pl.multiple_of((zz * TP + tt) * R + c * RC, RC)
        return T.at[pl.ds(start, RC), :]

    def t_line(zz, way, c):
        place = t_rows(zz, tp, c)
        to = (z + 1 - 2 * way) * Y + y
        return remote(place, place, tz_send.at[way, zz, c], tz_recv.at[zz, c], to, tp)

    def t_side(zz, k, c, source):
        place = t_rows(zz, source, c)
        return remote(place, place, tx_send.at[k - 1, zz, c], tx_recv.at[k - 1, zz, c], sp, side_tp(k))

    def t_twin(zz, k, c, source):
        place = t_rows(zz, source, c)
        return remote(place, place, tt_send.at[k, zz, c], tt_recv.at[k, zz, c], sp, twin)

    def o_rows(zz, yy, c):
        start = pl.multiple_of((zz * Y + yy) * KO + c * RO, RO)
        return O.at[pl.ds(start, RO), :]

    def o_line(zz, way, c, own):
        place = o_rows(zz, y, c)
        src = w_out.at[pl.ds(c * RO, RO), :] if own else place
        to = (z + 1 - 2 * way) * Y + y
        return remote(src, place, oz_send.at[way, zz, c], oz_recv.at[zz, c], to, tp)

    def o_side(zz, k, c, source, own):
        place = o_rows(zz, source, c)
        src = w_out.at[pl.ds(c * RO, RO), :] if own else place
        return remote(src, place, oy_send.at[k - 1, zz, c], oy_recv.at[k - 1, zz, c], z * Y + up_y(k), tp)

    def h_side(zz, shift):
        rows = pl.ds(pl.multiple_of(zz * N + N - WINDOW, WINDOW), WINDOW)
        return remote(
            PROJ.at[rows, pl.ds(3 * LANES, LANES)], HALO.at[zz + shift],
            h_send.at[zz], h_recv.at[zz], z * Y + up_y(1), tp,
        )

    def s_side(zz, k, source):
        place = ST.at[zz * Y + source]
        return remote(place, place, s_send.at[k - 1, zz], s_recv.at[k - 1, zz], z * Y + up_y(k), tp)

    def j_across(k, source):
        return remote(JS.at[up_z(k)], J.at[tp, source], jz_send.at[k], jz_recv.at[k], up_z(k) * Y + y, tp)

    def l_across(k, source):
        return remote(LS.at[up_z(k)], LT.at[source], l_send.at[k], l_recv.at[k], up_z(k) * Y + y, tp)

    def j_side(zz, k, source):
        place = J.at[source, zz]
        return remote(place, place, jx_send.at[k - 1, zz], jx_recv.at[k - 1, zz], sp, side_tp(k))

    def j_twin(zz, k, source):
        place = J.at[source, zz]
        return remote(place, place, jt_send.at[k, zz], jt_recv.at[k, zz], sp, twin)

    keep = [
        pltpu.make_async_copy(packed.at[z], w_rows(z, y), own_sems.at[0]),
        pltpu.make_async_copy(gate_cols, GW, own_sems.at[1]),
        pltpu.make_async_copy(
            w_out, O.at[pl.ds(pl.multiple_of(sp * KO, KO), KO), :], own_sems.at[2]
        ),
    ]

    barrier = pltpu.get_barrier_semaphore()
    greeted = [(up_z(k) * Y + y, tp) for k in range(1, Z)]
    greeted += [(z * Y + up_y(k), tp) for k in range(1, Y)]
    greeted += [(sp, side_tp(k)) for k in range(1, XH)] + [(sp, twin)]
    for to_sp, to_tp in greeted:
        pl.semaphore_signal(
            barrier, inc=1, device_id={"sp": to_sp, "tp": to_tp}, device_id_type=MESH
        )
    for copy in keep:
        copy.start()

    step = 16
    for i in range(R // step):
        values = tokens[pl.ds(i * step, step), :].astype(jnp.float32)
        rescale = lax.rsqrt(jnp.mean(values * values, axis=-1, keepdims=True) + EPSILON)
        start = pl.multiple_of((z * TP + tp) * R + i * step, step)
        T[pl.ds(start, step), :] = (values * rescale * gain[...]).astype(jnp.bfloat16)
    FS[z] = shifts[z]

    @pl.when(y == 0)
    def _():
        HALO[0] = jnp.zeros(HALO.shape[1:], HALO.dtype)

    pl.semaphore_wait(barrier, len(greeted))

    def weights_out(act):
        for k in range(1, Z):
            act(w_across(k, z))
            act(f_across(k, z))
        for j in range(1, Y):
            act(w_side(0, j, y))

    def own_tokens(act):
        for c in range(TC):
            pl.when(can_up)(lambda: act(t_line(z, 0, c)))
            pl.when(can_down)(lambda: act(t_line(z, 1, c)))
            for k in range(1, XH):
                act(t_side(z, k, c, tp))
            act(t_twin(z, 0, c, tp))

    def weights_on(act):
        for k in range(1, Z):
            if act is begin:
                w_across(k, back_z(k)).wait_recv()
            for j in range(1, Y):
                act(w_side(k, j, y))

    def tokens_on(d, act):
        for way, origin, there, further in (
            (0, z - d, z - d >= 0, can_up), (1, z + d, z + d < Z, can_down),
        ):
            def landed(way=way, origin=origin, further=further):
                for c in range(TC):
                    if act is begin:
                        t_line(origin, way, c).wait_recv()
                    pl.when(further)(lambda: act(t_line(origin, way, c)))
                    for k in range(1, XH):
                        act(t_side(origin, k, c, tp))
                    act(t_twin(origin, 0, c, tp))

            pl.when(there)(landed)

    def tokens_aside(zz, act):
        for k in range(1, XH):
            for c in range(TC):
                if act is begin:
                    t_side(zz, k, c, from_tp(k)).wait_recv()
                act(t_twin(zz, k, c, from_tp(k)))

    def own_output(act):
        for c in range(OC):
            pl.when(can_up)(lambda: act(o_line(z, 0, c, True)))
            pl.when(can_down)(lambda: act(o_line(z, 1, c, True)))
            for k in range(1, Y):
                act(o_side(z, k, c, y, True))

    def output_on(d, act):
        for way, origin, there, further in (
            (0, z - d, z - d >= 0, can_up), (1, z + d, z + d < Z, can_down),
        ):
            def landed(way=way, origin=origin, further=further):
                for c in range(OC):
                    if act is begin:
                        o_line(origin, way, c, False).wait_recv()
                    pl.when(further)(lambda: act(o_line(origin, way, c, False)))
                    for k in range(1, Y):
                        act(o_side(origin, k, c, y, False))

            pl.when(there)(landed)

    def block_rows(zz):
        return pl.ds(pl.multiple_of(zz * N, N), N)

    depth = 1024

    def project(zz):
        ACC[...] = jnp.zeros_like(ACC)

        def part(i, nothing):
            cols = pl.ds(pl.multiple_of(i * depth, depth), depth)
            block = T[block_rows(zz), cols]
            ACC[:, :C] += dot(block, W[cols, :])
            ACC[:, C:] += dot(block, GW[cols, :])
            return nothing

        lax.fori_loop(0, D // depth, part, 0)
        PROJ[block_rows(zz), :] = ACC[:, :C].astype(jnp.bfloat16)

    parts = N // WINDOW
    wide = (WINDOW, LANES)

    def sub_rows(zz, i):
        return pl.ds(pl.multiple_of(zz * N + i * WINDOW, WINDOW), WINDOW)

    def attend(zz, i, before):
        lane = lanes_of(wide)
        heads = PROJ[sub_rows(zz, i), :LANES].astype(jnp.float32) * HD ** (-0.5)
        first = jnp.where(lane < HD, heads, 0.0)
        second = jnp.where(lane < HD, pltpu.roll(heads, HD, 1), 0.0)
        query = jnp.concatenate([first, second], axis=0).astype(jnp.bfloat16)
        rows = jnp.concatenate([before, PROJ[sub_rows(zz, i), 3 * LANES :]], axis=0)
        scores = lax.dot_general(
            query, rows, (((1,), (1,)), ((), ())), preferred_element_type=jnp.float32
        )
        shape = (2 * WINDOW, 2 * WINDOW)
        at = lax.broadcasted_iota(jnp.int32, shape, 0)
        head = at >= WINDOW
        key_at = lax.broadcasted_iota(jnp.int32, shape, 1)
        distance = jnp.where(head, at - WINDOW, at) - key_at + WINDOW
        allowed = (distance >= 0) & (distance < WINDOW)
        if i == 0:
            lowest = WINDOW * (1 - jnp.minimum(zz * Y + y, 1))
            allowed = allowed & (key_at >= lowest)
        scores = jnp.where(allowed, scores, MASKED)
        tall = lax.broadcasted_iota(jnp.int32, (2 * WINDOW, 1), 0) >= WINDOW
        sink = jnp.where(tall, sinks[2 * z + 1], sinks[2 * z])
        ceiling = jnp.maximum(jnp.max(scores, axis=-1, keepdims=True), sink)
        weights = jnp.exp(scores - ceiling)
        total = jnp.exp(sink - ceiling) + jnp.sum(weights, axis=-1, keepdims=True)
        probs = (weights * (1.0 / total)).astype(jnp.bfloat16)
        out = dot(probs, rows)
        both = jnp.where(lane < HD, pltpu.roll(out[:WINDOW], HD, 1), out[WINDOW:])
        JS[zz, pl.ds(i * WINDOW, WINDOW), :] = both.astype(jnp.bfloat16)
        logs = jnp.broadcast_to(ceiling + jnp.log(total), (2 * WINDOW, LANES)).T
        LS[zz, 0:1, pl.ds(i * WINDOW, WINDOW)] = logs[0:1, :WINDOW]
        LS[zz, 1:2, pl.ds(i * WINDOW, WINDOW)] = logs[0:1, WINDOW:]

    def remember(zz):
        flat = ACC[:, C:].T
        log_in = flat[0:1, :] - 0.5 * math.log(N * S)
        pre = flat[1:2, :] + bias[z]
        log_sig = jnp.minimum(pre, 0.0) - jnp.log1p(jnp.exp(-jnp.abs(pre)))
        log_forget = log_sig + FS[zz][0:1, :]
        square = (N, N)
        before = lax.broadcasted_iota(jnp.int32, square, 0) <= lax.broadcasted_iota(
            jnp.int32, square, 1
        )
        summed = dot(
            jnp.broadcast_to(log_forget, (8, N)), before.astype(jnp.float32),
            precision=lax.Precision.HIGHEST,
        )[0:1, :]
        passed = summed[:, N - 1 :]
        decays = passed - summed + log_in
        level = jnp.max(decays, axis=1, keepdims=True)
        weights = jnp.exp(decays - level)
        pair = PROJ[block_rows(zz), LANES : 2 * LANES].astype(jnp.float32)
        query = (pair[:, :HD] * HD ** (-0.5)).astype(jnp.bfloat16)
        keys = pair.T[HD:, :]
        lane = lanes_of((N, LANES))
        values = PROJ[block_rows(zz), 2 * LANES : 3 * LANES].astype(jnp.float32)
        values = jnp.where(lane < HD, values, jnp.where(lane == HD, 1.0, 0.0)).astype(jnp.bfloat16)
        state = dot((keys * weights).astype(jnp.bfloat16), values)
        lane = lanes_of(state.shape)
        state = jnp.where(lane == HD + 1, passed, jnp.where(lane == HD + 2, level, state))
        ST[zz * Y + y] = state
        for k in range(1, Y):
            s_side(zz, k, y).start()
        keys = keys.astype(jnp.bfloat16)
        summed_col = jnp.broadcast_to(summed, (LANES, N)).T
        source = log_in - summed
        lane = lanes_of(wide)
        for i in range(parts):
            width = (i + 1) * WINDOW
            span = (WINDOW, width)
            causal = lax.broadcasted_iota(jnp.int32, span, 0) + i * WINDOW >= lanes_of(span)
            since = summed_col[i * WINDOW : (i + 1) * WINDOW, :]
            log_weight = jnp.where(causal, since[:, :1] + source[:, :width], MASKED)
            peak = jnp.max(log_weight, axis=-1, keepdims=True)
            affinity = dot(query[i * WINDOW : (i + 1) * WINDOW], keys[:, :width]) * jnp.exp(
                log_weight - peak
            )
            total = jnp.sum(affinity, axis=-1, keepdims=True)
            found = dot(affinity.astype(jnp.bfloat16), values[:width])
            NUM[sub_rows(zz, i), :] = jnp.where(
                lane < HD, found,
                jnp.where(lane == HD, total, jnp.where(lane == HD + 1, peak, since)),
            )

    def local_work(zz):
        project(zz)
        h_side(zz, (y + 1) // Y).start()
        remember(zz)
        for i in range(1, parts):
            attend(zz, i, PROJ[sub_rows(zz, i - 1), 3 * LANES :])

    weights_out(begin)
    own_tokens(begin)
    weights_on(begin)
    for k in range(1, Z):
        f_across(k, back_z(k)).wait_recv()
    for k in range(Z):
        for j in range(1, Y):
            w_side(k, j, back_y(j)).wait_recv()
    keep[0].wait()
    keep[1].wait()

    def stage(i, nothing):
        @pl.when(i == 1)
        def _():
            tokens_on(1, begin)

        @pl.when((i >= 1) & (i + 1 < Z))
        def _():
            tokens_on(i + 1, begin)

        @pl.when(i == Z - 1)
        def _():
            own_output(begin)

        def one(side, nothing):
            zz = z + i * (2 * side - 1)

            @pl.when((zz >= 0) & (zz < Z) & (i + 1 - side > 0))
            def _():
                tokens_aside(zz, begin)
                for k in range(XH):
                    for c in range(TC):
                        t_twin(zz, k, c, (twin + TP - 2 * k) % TP).wait_recv()
                local_work(zz)

            return nothing

        lax.fori_loop(0, 2, one, 0)
        return nothing

    lax.fori_loop(0, Z, stage, 0)

    output_on(1, begin)

    for zz in range(Z):
        h_side(zz, 1 - jnp.minimum(y, 1)).wait_recv()
        for k in range(1, Y):
            s_side(zz, k, back_y(k)).wait_recv()

    def enter():
        carried = jnp.zeros((HD, LANES), jnp.float32)
        stabilizer = jnp.full((1, 1), MASKED, jnp.float32)
        lane = lanes_of((HD, LANES))
        for i in range(S):
            @pl.when(y == i % Y)
            def _(carried=carried, stabilizer=stabilizer):
                EB[i // Y] = jnp.where(lane == HD + 1, stabilizer, carried)

            state = ST[i]
            passed, level = state[0:1, HD + 1 : HD + 2], state[0:1, HD + 2 : HD + 3]
            newer = jnp.maximum(stabilizer + passed, level)
            carried = carried * jnp.exp(stabilizer + passed - newer) + state * jnp.exp(level - newer)
            stabilizer = newer

    enter()

    def finish(zz):
        attend(zz, 0, HALO[zz])
        entering = EB[zz]
        stabilizer = entering[0:1, HD + 1 : HD + 2]
        local = NUM[block_rows(zz), :]
        peak, since = local[:, HD + 1 : HD + 2], local[:, HD + 2 : HD + 3]
        pair = PROJ[block_rows(zz), LANES : 2 * LANES].astype(jnp.float32)
        query = (pair[:, :HD] * HD ** (-0.5)).astype(jnp.bfloat16)
        carried = dot(query, entering.astype(jnp.bfloat16))
        older = since + stabilizer
        row_level = jnp.maximum(older, peak)
        found = jnp.exp(older - row_level) * carried + jnp.exp(peak - row_level) * local
        bound = jnp.maximum(jnp.abs(found[:, HD : HD + 1]), jnp.exp(-row_level))
        gate = pltpu.roll(
            PROJ[block_rows(zz), 2 * LANES : 3 * LANES].astype(jnp.float32), HD, 1
        )
        recall = found / bound * jax.nn.sigmoid(gate)
        half = N // 2
        lane = lanes_of((half, LANES))
        paired = jnp.where(lane < HD, recall[:half], pltpu.roll(recall[half:], HD, 1))
        JS[zz, N:, :] = paired.astype(jnp.bfloat16)

    def hand_over(act):
        for k in range(1, Z):
            act(j_across(k, z))
            act(l_across(k, z))

    for k in range(1, Z):
        finish(up_z(k))
        j_across(k, z).start()
        l_across(k, z).start()
        if k > 1:
            output_on(k, begin)
    finish(z)
    J[tp, z] = JS[z]
    LT[z] = LS[z]

    def share(act):
        for k in range(Z):
            zz = back_z(k)
            if k and act is begin:
                j_across(k, zz).wait_recv()
            for j in range(1, XH):
                act(j_side(zz, j, tp))
            act(j_twin(zz, 0, tp))
        for k in range(Z):
            zz = back_z(k)
            for j in range(1, XH):
                if act is begin:
                    j_side(zz, j, from_tp(j)).wait_recv()
                act(j_twin(zz, j, from_tp(j)))

    share(begin)
    for k in range(1, Z):
        l_across(k, back_z(k)).wait_recv()
    for k in range(XH):
        for zz in range(Z):
            j_twin(zz, k, (twin + TP - 2 * k) % TP).wait_recv()

    mem_base = TP * sinks.shape[0] * HD
    per_tp = sinks.shape[0] * HD
    half = N // 2
    LTF[...] = jnp.zeros_like(LTF)
    for zz in range(Z):
        for t in range(TP):
            at = t * per_tp + zz * LANES
            X[:, at : at + LANES] = J[t, zz, :N, :]
            at = mem_base + (t * Z + zz) * HD
            X[:half, at : at + HD] = J[t, zz, N:, :HD]
            X[half:, at : at + HD] = J[t, zz, N:, HD:]
        LTF[2 * zz : 2 * zz + 2, :] = LT[zz, 0:2, :]
    totals[...] = LTF[...].T[:, : sinks.shape[0]]

    keep[2].wait()
    for zz in range(Z):
        for k in range(1, Y):
            for c in range(OC):
                o_side(zz, k, c, back_y(k), False).wait_recv()

    tile = 256

    def columns(i, nothing):
        cols = pl.ds(pl.multiple_of(i * tile, tile), tile)
        mixed[:, cols] = dot(X[...], O[:, cols]).astype(jnp.bfloat16)
        return nothing

    lax.fori_loop(0, mixed.shape[1] // tile, columns, 0)

    weights_out(drain)
    own_tokens(drain)
    weights_on(drain)
    own_output(drain)

    def settle(i, nothing):
        tokens_on(i, drain)
        output_on(i, drain)
        return nothing

    lax.fori_loop(1, Z, settle, 0)
    for zz in range(Z):
        tokens_aside(zz, drain)
        h_side(zz, (y + 1) // Y).wait_send()
        for k in range(1, Y):
            s_side(zz, k, y).wait_send()
    hand_over(drain)
    share(drain)


def mix(tokens, gain, packed, shifts, gate_cols, w_out, sinks, bias):
    S, TP = lax.axis_size("sp"), lax.axis_size("tp")
    Z = packed.shape[0]
    Y, XH = S // Z, TP // 2
    R, D = tokens.shape
    N = R * TP
    C = packed.shape[2]
    TC = OC = 3
    M = w_out.shape[1]
    bf, f32 = jnp.bfloat16, jnp.float32
    dma = pltpu.SemaphoreType.DMA
    piece = N + N // 2
    vmem = pl.BlockSpec(memory_space=pltpu.VMEM)
    smem = pl.BlockSpec(memory_space=pltpu.SMEM)
    hbm = pl.BlockSpec(memory_space=pl.ANY)
    return pl.pallas_call(
        functools.partial(mixer_kernel, (Z, Y, TP, TC, OC)),
        out_shape=[
            jax.ShapeDtypeStruct((N, M), bf),
            jax.ShapeDtypeStruct((N, sinks.shape[0]), f32),
        ],
        in_specs=[vmem, vmem, hbm, vmem, hbm, hbm, smem, smem],
        out_specs=[vmem, vmem],
        scratch_shapes=[
            pltpu.VMEM((Z * N, D), bf),
            pltpu.VMEM((D, C), bf),
            pltpu.VMEM((D, LANES), bf),
            pltpu.VMEM((S * w_out.shape[0], M), bf),
            pltpu.VMEM((N, C + LANES), f32),
            pltpu.VMEM((Z * N, C), bf),
            pltpu.VMEM((Z * N, LANES), f32),
            pltpu.VMEM((S, HD, LANES), f32),
            pltpu.VMEM((Z, HD, LANES), f32),
            pltpu.VMEM((Z + 1, WINDOW, LANES), bf),
            pltpu.VMEM((Z, 8, N), f32),
            pltpu.VMEM((Z, piece, LANES), bf),
            pltpu.VMEM((TP, Z, piece, LANES), bf),
            pltpu.VMEM((Z, 8, N), f32),
            pltpu.VMEM((Z, 8, N), f32),
            pltpu.VMEM((LANES, N), f32),
            pltpu.VMEM((N, S * w_out.shape[0]), bf),
            dma((3,)),
            dma((Z,)), dma((Z,)), dma((Z, Y - 1)), dma((Z, Y - 1)), dma((Z,)), dma((Z,)),
            dma((2, Z, TC)), dma((Z, TC)), dma((XH - 1, Z, TC)), dma((XH - 1, Z, TC)),
            dma((XH, Z, TC)), dma((XH, Z, TC)),
            dma((2, Z, OC)), dma((Z, OC)), dma((Y - 1, Z, OC)), dma((Y - 1, Z, OC)),
            dma((Z,)), dma((Z,)), dma((Y - 1, Z)), dma((Y - 1, Z)),
            dma((Z,)), dma((Z,)), dma((Z,)), dma((Z,)),
            dma((XH - 1, Z)), dma((XH - 1, Z)), dma((XH, Z)), dma((XH, Z)),
        ],
        compiler_params=pltpu.CompilerParams(
            collective_id=0, has_side_effects=True, vmem_limit_bytes=60 * 2**20
        ),
    )(tokens, gain, packed, shifts, gate_cols, w_out, sinks, bias)


def shards(
    tokens,
    norm_gain,
    w_query,
    w_key,
    w_value,
    w_mem_query,
    w_mem_key,
    w_mem_value,
    w_mem_gate,
    w_gates,
    sinks,
    forget_bias,
    forget_shift,
    w_out,
):
    mem_heads = forget_bias.shape[0]
    Z = mem_heads
    Y = lax.axis_size("sp") // Z
    z, tp = lax.axis_index("sp") // Y, lax.axis_index("tp")
    q_width = w_query.shape[1] // Z
    per_z = q_width // HD
    group = w_query.shape[1] // w_key.shape[1]

    def piece(i):
        kv = i * per_z // group * HD
        mem = [
            part[:, i * HD : (i + 1) * HD]
            for part in (w_mem_query, w_mem_key, w_mem_value, w_mem_gate)
        ]
        return jnp.concatenate(
            [w_query[:, i * q_width : (i + 1) * q_width]]
            + mem
            + [w_key[:, kv : kv + HD], w_value[:, kv : kv + HD]],
            axis=1,
        )

    packed = jnp.stack([piece(i) for i in range(Z)])
    head = tp * mem_heads + z
    gate_cols = lax.dynamic_slice_in_dim(w_gates, head, 1, 2)[:, :, 0]
    gate_cols = jnp.pad(gate_cols, ((0, 0), (0, LANES - 2)))
    shifts = jnp.pad(forget_shift.T[:, None, :], ((0, 0), (0, 7), (0, 0)))
    mixed, totals = mix(
        tokens, norm_gain[None, :], packed, shifts, gate_cols, w_out, sinks, forget_bias
    )
    return mixed, totals


def solution(mesh):
    placed = (
        P(("sp", "tp"), None),
        P(),
        P("sp", "tp"),
        P("sp", "tp"),
        P("sp", "tp"),
        P("sp", "tp"),
        P("sp", "tp"),
        P("sp", "tp"),
        P("sp", "tp"),
        P(),
        P("tp"),
        P("tp"),
        P("sp", "tp"),
        P("sp", "tp"),
    )
    return jax.shard_map(
        shards,
        mesh=mesh,
        in_specs=placed,
        out_specs=(P("sp", "tp"), P("sp", "tp")),
        check_vma=False,
    )
```

```python
import functools
import math

import jax
import jax.numpy as jnp
from jax import lax
from jax.experimental import pallas as pl
from jax.experimental.pallas import tpu as pltpu
from jax.sharding import PartitionSpec as P

HD = 64
WINDOW = 128
LANES = 128
EPSILON = 1e-06
MASKED = -1e30
MESH = pl.DeviceIdType.MESH


def begin(copy):
    copy.start()


def drain(copy):
    copy.wait_send()


def dot(left, right, **more):
    return jnp.dot(left, right, preferred_element_type=jnp.float32, **more)


def lanes_of(shape):
    return lax.broadcasted_iota(jnp.int32, shape, len(shape) - 1)


def mixer_kernel(
    sizes,
    tokens, gain, shifts, gates, w_out, w_query, w_key, w_value, w_mem_query, w_mem_key,
    w_mem_value, w_mem_gate, sinks, bias,
    mixed, totals,
    in_query, in_key, in_value, in_mem_query, in_mem_key, in_mem_value, in_mem_gate,
    PACK, T, W, GW, O, ACC, FLAT, PROJ, NUM, ST, EB, HALO, SH, FS, JS, J, LS, LT, X,
    own_sems, w_send, w_recv, wy_send, wy_recv, f_send, f_recv,
    tz_send, tz_recv, tx_send, tx_recv, tt_send, tt_recv,
    oz_send, oz_recv, oy_send, oy_recv,
    h_send, h_recv, s_send, s_recv,
    jz_send, jz_recv, l_send, l_recv, jx_send, jx_recv, jt_send, jt_recv,
):
    Z, Y, TP, TC, WC, OC = sizes
    XH = TP // 2
    R, D = tokens.shape
    N = R * TP
    KD, C = PACK.shape[1:]
    KO = w_out.shape[0]
    RC, RW, RO = R // TC, KD // WC, KO // OC
    S = Z * Y
    sp, tp = lax.axis_index("sp"), lax.axis_index("tp")
    z, y = sp // Y, sp % Y
    twin = tp + 1 - 2 * (tp % 2)
    can_up, can_down = z < Z - 1, z > 0

    def remote(src, dst, send, recv, to_sp, to_tp):
        return pltpu.make_async_remote_copy(
            src_ref=src, dst_ref=dst, send_sem=send, recv_sem=recv,
            device_id={"sp": to_sp, "tp": to_tp}, device_id_type=MESH,
        )

    def side_tp(k):
        return (tp + 2 * k) % TP

    def from_tp(k):
        return (tp + TP - 2 * k) % TP

    def up_z(k):
        return (z + k) % Z

    def back_z(k):
        return (z + Z - k) % Z

    def up_y(k):
        return (y + k) % Y

    def back_y(k):
        return (y + Y - k) % Y

    def w_rows(zz, yy, c):
        return W.at[pl.ds(pl.multiple_of((zz * Y + yy) * KD + c * RW, RW), RW), :]

    def w_across(way, d, c):
        to = z + d * (1 - 2 * way)
        return remote(
            PACK.at[to, pl.ds(c * RW, RW), :], w_rows(z, y, c),
            w_send.at[way, d, c], w_recv.at[way, d, c], to * Y + y, tp,
        )

    def w_landed(way, d, c):
        origin = z - d * (1 - 2 * way)
        return remote(
            PACK.at[z, pl.ds(c * RW, RW), :], w_rows(origin, y, c),
            w_send.at[way, d, c], w_recv.at[way, d, c], sp, tp,
        )

    def w_side(zz, j, c, source):
        place = w_rows(zz, source, c)
        return remote(
            place, place, wy_send.at[j - 1, zz, c], wy_recv.at[j - 1, zz, c], z * Y + up_y(j), tp
        )

    def f_across(k, source):
        return remote(
            SH.at[up_z(k)], FS.at[source], f_send.at[k], f_recv.at[k], up_z(k) * Y + y, tp
        )

    def t_rows(zz, tt, c):
        start = pl.multiple_of((zz * TP + tt) * R + c * RC, RC)
        return T.at[pl.ds(start, RC), :]

    def t_line(zz, way, c):
        place = t_rows(zz, tp, c)
        to = (z + 1 - 2 * way) * Y + y
        return remote(place, place, tz_send.at[way, zz, c], tz_recv.at[zz, c], to, tp)

    def t_side(zz, k, c, source):
        place = t_rows(zz, source, c)
        return remote(place, place, tx_send.at[k - 1, zz, c], tx_recv.at[k - 1, zz, c], sp, side_tp(k))

    def t_twin(zz, k, c, source):
        place = t_rows(zz, source, c)
        return remote(place, place, tt_send.at[k, zz, c], tt_recv.at[k, zz, c], sp, twin)

    def o_rows(zz, yy, c):
        start = pl.multiple_of((zz * Y + yy) * KO + c * RO, RO)
        return O.at[pl.ds(start, RO), :]

    def o_line(zz, way, c, own):
        place = o_rows(zz, y, c)
        src = w_out.at[pl.ds(c * RO, RO), :] if own else place
        to = (z + 1 - 2 * way) * Y + y
        return remote(src, place, oz_send.at[way, zz, c], oz_recv.at[zz, c], to, tp)

    def o_side(zz, k, c, source, own):
        place = o_rows(zz, source, c)
        src = w_out.at[pl.ds(c * RO, RO), :] if own else place
        return remote(src, place, oy_send.at[k - 1, zz, c], oy_recv.at[k - 1, zz, c], z * Y + up_y(k), tp)

    def h_side(zz, shift):
        rows = pl.ds(pl.multiple_of(zz * N + N - WINDOW, WINDOW), WINDOW)
        return remote(
            PROJ.at[rows, pl.ds(3 * LANES, LANES)], HALO.at[zz + shift],
            h_send.at[zz], h_recv.at[zz], z * Y + up_y(1), tp,
        )

    def s_side(zz, k, source):
        place = ST.at[zz * Y + source]
        return remote(place, place, s_send.at[k - 1, zz], s_recv.at[k - 1, zz], z * Y + up_y(k), tp)

    def j_across(k, source):
        return remote(JS.at[up_z(k)], J.at[tp, source], jz_send.at[k], jz_recv.at[k], up_z(k) * Y + y, tp)

    def l_across(k, source):
        return remote(LS.at[up_z(k)], LT.at[source], l_send.at[k], l_recv.at[k], up_z(k) * Y + y, tp)

    def j_side(zz, k, source):
        place = J.at[source, zz]
        return remote(place, place, jx_send.at[k - 1, zz], jx_recv.at[k - 1, zz], sp, side_tp(k))

    def j_twin(zz, k, source):
        place = J.at[source, zz]
        return remote(place, place, jt_send.at[k, zz], jt_recv.at[k, zz], sp, twin)

    ins = (
        (w_query, in_query), (w_key, in_key), (w_value, in_value), (w_mem_query, in_mem_query),
        (w_mem_key, in_mem_key), (w_mem_value, in_mem_value), (w_mem_gate, in_mem_gate),
        (gates, GW), (w_out, O.at[pl.ds(pl.multiple_of(sp * KO, KO), KO), :]),
    )
    keep = [pltpu.make_async_copy(a, b, own_sems.at[i]) for i, (a, b) in enumerate(ins)]

    barrier = pltpu.get_barrier_semaphore()
    greeted = [(up_z(k) * Y + y, tp) for k in range(1, Z)]
    greeted += [(z * Y + up_y(k), tp) for k in range(1, Y)]
    greeted += [(sp, side_tp(k)) for k in range(1, XH)] + [(sp, twin)]
    for to_sp, to_tp in greeted:
        pl.semaphore_signal(
            barrier, inc=1, device_id={"sp": to_sp, "tp": to_tp}, device_id_type=MESH
        )
    for copy in keep:
        copy.start()

    step = 16
    for i in range(R // step):
        values = tokens[pl.ds(i * step, step), :].astype(jnp.float32)
        rescale = lax.rsqrt(jnp.mean(values * values, axis=-1, keepdims=True) + EPSILON)
        start = pl.multiple_of((z * TP + tp) * R + i * step, step)
        T[pl.ds(start, step), :] = (values * rescale * gain[...]).astype(jnp.bfloat16)
    for i in range(Z):
        SH[i, 0:1, :] = shifts[i : i + 1, :]
    FS[z] = SH[z]

    @pl.when(y == 0)
    def _():
        HALO[0] = jnp.zeros(HALO.shape[1:], HALO.dtype)

    with jax.named_scope('barrier_wait'):
        pl.semaphore_wait(barrier, len(greeted))

    def pack():
        for copy in keep[:7]:
            copy.wait()
        group = w_query.shape[1] // w_key.shape[1]
        high = min(KD, WINDOW)
        lane = lanes_of((high, LANES))

        def halves(rows, left, i, right, j):
            a = left[rows, pl.ds(i // 2 * LANES, LANES)].astype(jnp.float32)
            b = right[rows, pl.ds(j // 2 * LANES, LANES)].astype(jnp.float32)
            a = pltpu.roll(a, HD, 1) if i % 2 else a
            b = b if j % 2 else pltpu.roll(b, HD, 1)
            return jnp.where(lane < HD, a, b).astype(jnp.bfloat16)

        def some(r, nothing):
            rows = pl.ds(pl.multiple_of(r * high, high), high)
            for i in range(Z):
                kv = i * (LANES // HD) // group
                PACK[i, rows, :LANES] = in_query[rows, i * LANES : (i + 1) * LANES]
                for n, parts in enumerate(
                    (
                        (in_mem_query, i, in_mem_key, i),
                        (in_mem_value, i, in_mem_gate, i),
                        (in_key, kv, in_value, kv),
                    )
                ):
                    PACK[i, rows, (n + 1) * LANES : (n + 2) * LANES] = halves(rows, *parts)
            return nothing

        lax.fori_loop(0, KD // high, some, 0)
        W[pl.ds(pl.multiple_of(sp * KD, KD), KD), :] = PACK[z]

    def ways(d):
        return ((0, z + d < Z, z - d >= 0), (1, z - d >= 0, z + d < Z))

    def weights_out(way, d, act):
        for c in range(WC):
            act(w_across(way, d, c))

    def weights_far(act):
        for d in range(2, Z):
            for way, there, _ in ways(d):
                pl.when(there)(lambda: weights_out(way, d, act))

    def weights_aside(zz, act):
        for c in range(WC):
            for j in range(1, Y):
                act(w_side(zz, j, c, y))

    def weights_on(d, act):
        for way, _, there in ways(d):
            def landed(way=way):
                for c in range(WC):
                    if act is begin:
                        w_landed(way, d, c).wait_recv()
                    for j in range(1, Y):
                        act(w_side(z - d * (1 - 2 * way), j, c, y))

            pl.when(there)(landed)

    def own_tokens(act):
        for c in range(TC):
            pl.when(can_up)(lambda: act(t_line(z, 0, c)))
            pl.when(can_down)(lambda: act(t_line(z, 1, c)))
            for k in range(1, XH):
                act(t_side(z, k, c, tp))
            act(t_twin(z, 0, c, tp))

    def tokens_on(d, act):
        for way, origin, there, further in (
            (0, z - d, z - d >= 0, can_up), (1, z + d, z + d < Z, can_down),
        ):
            def landed(way=way, origin=origin, further=further):
                for c in range(TC):
                    if act is begin:
                        t_line(origin, way, c).wait_recv()
                    pl.when(further)(lambda: act(t_line(origin, way, c)))
                    for k in range(1, XH):
                        act(t_side(origin, k, c, tp))
                    act(t_twin(origin, 0, c, tp))

            pl.when(there)(landed)

    def tokens_aside(zz, act):
        for k in range(1, XH):
            for c in range(TC):
                if act is begin:
                    t_side(zz, k, c, from_tp(k)).wait_recv()
                act(t_twin(zz, k, c, from_tp(k)))

    def output_aside(act):
        for c in range(OC):
            for k in range(1, Y):
                act(o_side(z, k, c, y, True))

    def own_output(act):
        for c in range(OC):
            pl.when(can_up)(lambda: act(o_line(z, 0, c, True)))
            pl.when(can_down)(lambda: act(o_line(z, 1, c, True)))

    def output_on(d, act):
        for way, origin, there, further in (
            (0, z - d, z - d >= 0, can_up), (1, z + d, z + d < Z, can_down),
        ):
            def landed(way=way, origin=origin, further=further):
                for c in range(OC):
                    if act is begin:
                        o_line(origin, way, c, False).wait_recv()
                    pl.when(further)(lambda: act(o_line(origin, way, c, False)))
                    for k in range(1, Y):
                        act(o_side(origin, k, c, y, False))

            pl.when(there)(landed)

    def block_rows(zz):
        return pl.ds(pl.multiple_of(zz * N, N), N)

    depth = Y * KD

    def project(zk):
        cols = pl.ds(pl.multiple_of(zk * depth, depth), depth)

        def part(b, nothing):
            rows = block_rows(b)
            block = T[rows, cols]
            ACC[rows, :C] += dot(block, W[cols, :])
            ACC[rows, C : C + GW.shape[1]] += dot(block, GW[cols, :])
            return nothing

        lax.fori_loop(0, Z, part, 0)

    parts = N // WINDOW
    wide = (WINDOW, LANES)

    def sub_rows(zz, i):
        return pl.ds(pl.multiple_of(zz * N + i * WINDOW, WINDOW), WINDOW)

    def attend(zz, i, before):
        lane = lanes_of(wide)
        heads = PROJ[sub_rows(zz, i), :LANES].astype(jnp.float32) * HD ** (-0.5)
        first = jnp.where(lane < HD, heads, 0.0)
        second = jnp.where(lane < HD, pltpu.roll(heads, HD, 1), 0.0)
        query = jnp.concatenate([first, second], axis=0).astype(jnp.bfloat16)
        rows = jnp.concatenate([before, PROJ[sub_rows(zz, i), 3 * LANES :]], axis=0)
        scores = lax.dot_general(
            query, rows, (((1,), (1,)), ((), ())), preferred_element_type=jnp.float32
        )
        shape = (2 * WINDOW, 2 * WINDOW)
        at = lax.broadcasted_iota(jnp.int32, shape, 0)
        head = at >= WINDOW
        key_at = lax.broadcasted_iota(jnp.int32, shape, 1)
        distance = jnp.where(head, at - WINDOW, at) - key_at + WINDOW
        allowed = (distance >= 0) & (distance < WINDOW)
        if i == 0:
            lowest = WINDOW * (1 - jnp.minimum(zz * Y + y, 1))
            allowed = allowed & (key_at >= lowest)
        scores = jnp.where(allowed, scores, MASKED)
        tall = lax.broadcasted_iota(jnp.int32, (2 * WINDOW, 1), 0) >= WINDOW
        sink = jnp.where(tall, sinks[2 * z + 1], sinks[2 * z])
        ceiling = jnp.maximum(jnp.max(scores, axis=-1, keepdims=True), sink)
        weights = jnp.exp(scores - ceiling)
        total = jnp.exp(sink - ceiling) + jnp.sum(weights, axis=-1, keepdims=True)
        probs = (weights * (1.0 / total)).astype(jnp.bfloat16)
        out = dot(probs, rows)
        both = jnp.where(lane < HD, pltpu.roll(out[:WINDOW], HD, 1), out[WINDOW:])
        JS[zz, pl.ds(i * WINDOW, WINDOW), :] = both.astype(jnp.bfloat16)
        logs = jnp.broadcast_to(ceiling + jnp.log(total), (2 * WINDOW, LANES)).T
        LS[zz, 0:1, pl.ds(i * WINDOW, WINDOW)] = logs[0:1, :WINDOW]
        LS[zz, 1:2, pl.ds(i * WINDOW, WINDOW)] = logs[0:1, WINDOW:]

    def remember(zz):
        FLAT[...] = ACC[block_rows(zz), C:].T
        gate_count = GW.shape[1] // 2
        head = tp * Z + z
        log_in = FLAT[pl.ds(head, 1), :] - 0.5 * math.log(N * S)
        pre = FLAT[pl.ds(gate_count + head, 1), :] + bias[z]
        log_sig = jnp.minimum(pre, 0.0) - jnp.log1p(jnp.exp(-jnp.abs(pre)))
        log_forget = log_sig + FS[zz][0:1, :]
        square = (N, N)
        before = lax.broadcasted_iota(jnp.int32, square, 0) <= lax.broadcasted_iota(
            jnp.int32, square, 1
        )
        summed = dot(
            jnp.broadcast_to(log_forget, (8, N)), before.astype(jnp.float32),
            precision=lax.Precision.HIGHEST,
        )[0:1, :]
        passed = summed[:, N - 1 :]
        decays = passed - summed + log_in
        level = jnp.max(decays, axis=1, keepdims=True)
        weights = jnp.exp(decays - level)
        pair = PROJ[block_rows(zz), LANES : 2 * LANES].astype(jnp.float32)
        query = (pair[:, :HD] * HD ** (-0.5)).astype(jnp.bfloat16)
        keys = pair.T[HD:, :]
        lane = lanes_of((N, LANES))
        values = PROJ[block_rows(zz), 2 * LANES : 3 * LANES].astype(jnp.float32)
        values = jnp.where(lane < HD, values, jnp.where(lane == HD, 1.0, 0.0)).astype(jnp.bfloat16)
        state = dot((keys * weights).astype(jnp.bfloat16), values)
        lane = lanes_of(state.shape)
        state = jnp.where(lane == HD + 1, passed, jnp.where(lane == HD + 2, level, state))
        ST[zz * Y + y] = state
        keys = keys.astype(jnp.bfloat16)
        summed_col = jnp.broadcast_to(summed, (LANES, N)).T
        source = log_in - summed
        lane = lanes_of(wide)
        for i in range(parts):
            width = (i + 1) * WINDOW
            span = (WINDOW, width)
            causal = lax.broadcasted_iota(jnp.int32, span, 0) + i * WINDOW >= lanes_of(span)
            since = summed_col[i * WINDOW : (i + 1) * WINDOW, :]
            log_weight = jnp.where(causal, since[:, :1] + source[:, :width], MASKED)
            peak = jnp.max(log_weight, axis=-1, keepdims=True)
            affinity = dot(query[i * WINDOW : (i + 1) * WINDOW], keys[:, :width]) * jnp.exp(
                log_weight - peak
            )
            total = jnp.sum(affinity, axis=-1, keepdims=True)
            found = dot(affinity.astype(jnp.bfloat16), values[:width])
            NUM[sub_rows(zz, i), :] = jnp.where(
                lane < HD, found,
                jnp.where(lane == HD, total, jnp.where(lane == HD + 1, peak, since)),
            )

    def local_work(zz):
        PROJ[block_rows(zz), :] = ACC[block_rows(zz), :C].astype(jnp.bfloat16)
        with jax.named_scope('remember'):
            remember(zz)
        h_side(zz, (y + 1) // Y).start()
        with jax.named_scope('attend'):
            for i in range(1, parts):
                attend(zz, i, PROJ[sub_rows(zz, i - 1), 3 * LANES :])
        for k in range(1, Y):
            s_side(zz, k, y).start()

    own_tokens(begin)
    with jax.named_scope('pack'):
        pack()
    for k in range(1, Z):
        f_across(k, z).start()
    weights_aside(z, begin)
    output_aside(begin)
    ACC[...] = jnp.zeros_like(ACC)

    def both_sides(d, act):
        def one(side, nothing):
            zz = z + d * (2 * side - 1)
            pl.when((zz >= 0) & (zz < Z) & (d + 1 - side > 0))(lambda: act(zz))
            return nothing

        lax.fori_loop(0, 2, one, 0)

    def near(d, act):
        pl.when((z == d - 1) & can_up)(lambda: weights_out(0, 1, act))
        pl.when((z == Z - d) & can_down)(lambda: weights_out(1, 1, act))

    def stage(d, nothing):
        near(d, begin)
        with jax.named_scope('t_on'):
            tokens_on(d, begin)
        with jax.named_scope('t_aside'):
            both_sides(d - 1, lambda zz: tokens_aside(zz, begin))
        return nothing

    lax.fori_loop(1, Z, stage, 0)
    weights_far(begin)
    own_output(begin)
    with jax.named_scope('w_on_1'):
        weights_on(1, begin)
    with jax.named_scope('t_last'):
        both_sides(Z - 1, lambda zz: tokens_aside(zz, begin))
        for zz in range(Z):
            for k in range(XH):
                for c in range(TC):
                    t_twin(zz, k, c, (twin + TP - 2 * k) % TP).wait_recv()
    keep[7].wait()

    def multiply(zz):
        with jax.named_scope('w_side'):
            for j in range(1, Y):
                for c in range(WC):
                    w_side(zz, j, c, back_y(j)).wait_recv()
        with jax.named_scope('project'):
            project(zz)

    def stage_two(d, nothing):
        @pl.when((d > 0) & (d + 1 < Z))
        def _():
            with jax.named_scope('w_on'):
                weights_on(d + 1, begin)

        both_sides(d, multiply)
        return nothing

    lax.fori_loop(0, Z, stage_two, 0)
    for k in range(1, Z):
        f_across(k, back_z(k)).wait_recv()

    def local(zz, nothing):
        local_work(zz)
        return nothing

    lax.fori_loop(0, Z, local, 0)

    with jax.named_scope('halo_state'):
        for zz in range(Z):
            h_side(zz, 1 - jnp.minimum(y, 1)).wait_recv()
            for k in range(1, Y):
                s_side(zz, k, back_y(k)).wait_recv()

    def enter():
        carried = jnp.zeros((HD, LANES), jnp.float32)
        stabilizer = jnp.full((1, 1), MASKED, jnp.float32)
        lane = lanes_of((HD, LANES))
        for i in range(S):
            @pl.when(y == i % Y)
            def _(carried=carried, stabilizer=stabilizer):
                EB[i // Y] = jnp.where(lane == HD + 1, stabilizer, carried)

            state = ST[i]
            passed, level = state[0:1, HD + 1 : HD + 2], state[0:1, HD + 2 : HD + 3]
            newer = jnp.maximum(stabilizer + passed, level)
            carried = carried * jnp.exp(stabilizer + passed - newer) + state * jnp.exp(level - newer)
            stabilizer = newer

    enter()

    def finish(zz):
        attend(zz, 0, HALO[zz])
        entering = EB[zz]
        stabilizer = entering[0:1, HD + 1 : HD + 2]
        local = NUM[block_rows(zz), :]
        peak, since = local[:, HD + 1 : HD + 2], local[:, HD + 2 : HD + 3]
        pair = PROJ[block_rows(zz), LANES : 2 * LANES].astype(jnp.float32)
        query = (pair[:, :HD] * HD ** (-0.5)).astype(jnp.bfloat16)
        carried = dot(query, entering.astype(jnp.bfloat16))
        older = since + stabilizer
        row_level = jnp.maximum(older, peak)
        found = jnp.exp(older - row_level) * carried + jnp.exp(peak - row_level) * local
        bound = jnp.maximum(jnp.abs(found[:, HD : HD + 1]), jnp.exp(-row_level))
        gate = pltpu.roll(
            PROJ[block_rows(zz), 2 * LANES : 3 * LANES].astype(jnp.float32), HD, 1
        )
        recall = found / bound * jax.nn.sigmoid(gate)
        half = N // 2
        lane = lanes_of((half, LANES))
        paired = jnp.where(lane < HD, recall[:half], pltpu.roll(recall[half:], HD, 1))
        JS[zz, N:, :] = paired.astype(jnp.bfloat16)

    def hand_over(act):
        for k in range(1, Z):
            act(j_across(k, z))
            act(l_across(k, z))

    for k in range(1, Z):
        with jax.named_scope('finish'):
            finish(up_z(k))
        j_across(k, z).start()
        l_across(k, z).start()
    with jax.named_scope('finish'):
        finish(z)
    J[tp, z] = JS[z]
    LT[z] = LS[z]

    def share(act):
        for k in range(Z):
            zz = back_z(k)
            if k and act is begin:
                j_across(k, zz).wait_recv()
            for j in range(1, XH):
                act(j_side(zz, j, tp))
            act(j_twin(zz, 0, tp))

    def share_aside(act):
        for k in range(Z):
            zz = back_z(k)
            for j in range(1, XH):
                if act is begin:
                    j_side(zz, j, from_tp(j)).wait_recv()
                act(j_twin(zz, j, from_tp(j)))

    with jax.named_scope('o_on_1'):
        output_on(1, begin)
    with jax.named_scope('share'):
        share(begin)
    with jax.named_scope('o_on_2'):
        output_on(2, begin)
    with jax.named_scope('share_aside'):
        share_aside(begin)
    for d in range(3, Z):
        with jax.named_scope('o_on_3'):
            output_on(d, begin)
    with jax.named_scope('share_wait'):
        for k in range(1, Z):
            l_across(k, back_z(k)).wait_recv()
        for k in range(XH):
            for zz in range(Z):
                j_twin(zz, k, (twin + TP - 2 * k) % TP).wait_recv()

    mem_base = TP * sinks.shape[0] * HD
    per_tp = sinks.shape[0] * HD
    half = N // 2
    for zz in range(Z):
        for t in range(TP):
            at = t * per_tp + zz * LANES
            X[:, at : at + LANES] = J[t, zz, :N, :]
            at = mem_base + (t * Z + zz) * HD
            X[:half, at : at + HD] = J[t, zz, N:, :HD]
            X[half:, at : at + HD] = J[t, zz, N:, HD:]
        totals[2 * zz : 2 * zz + 2, :] = LT[zz, 0:2, :]

    with jax.named_scope('o_wait'):
        keep[8].wait()
        for zz in range(Z):
            for k in range(1, Y):
                for c in range(OC):
                    o_side(zz, k, c, back_y(k), False).wait_recv()

    tile = 256

    def columns(i, nothing):
        cols = pl.ds(pl.multiple_of(i * tile, tile), tile)
        mixed[:, cols] = dot(X[...], O[:, cols]).astype(jnp.bfloat16)
        return nothing

    with jax.named_scope('out_matmul'):
        lax.fori_loop(0, mixed.shape[1] // tile, columns, 0)

    own_tokens(drain)
    weights_far(drain)
    weights_aside(z, drain)
    output_aside(drain)
    own_output(drain)
    for k in range(1, Z):
        f_across(k, z).wait_send()

    def settle(i, nothing):
        near(i, drain)
        weights_on(i, drain)
        tokens_on(i, drain)
        output_on(i, drain)
        return nothing

    lax.fori_loop(1, Z, settle, 0)
    for zz in range(Z):
        tokens_aside(zz, drain)
        h_side(zz, (y + 1) // Y).wait_send()
        for k in range(1, Y):
            s_side(zz, k, y).wait_send()
    hand_over(drain)
    share(drain)
    share_aside(drain)


def mix(tokens, gain, shifts, gates, w_out, weights, sinks, bias):
    S, TP = lax.axis_size("sp"), lax.axis_size("tp")
    Z = shifts.shape[0]
    Y, XH = S // Z, TP // 2
    R, D = tokens.shape
    N = R * TP
    KD = weights[0].shape[0]
    C = sum(part.shape[1] for part in weights[3:]) // Z + weights[0].shape[1] // Z + 2 * HD
    TC = OC = 3
    WC = 2
    M = w_out.shape[1]
    bf, f32 = jnp.bfloat16, jnp.float32
    dma = pltpu.SemaphoreType.DMA
    piece = N + N // 2
    vmem = pl.BlockSpec(memory_space=pltpu.VMEM)
    smem = pl.BlockSpec(memory_space=pltpu.SMEM)
    hbm = pl.BlockSpec(memory_space=pl.ANY)
    return pl.pallas_call(
        functools.partial(mixer_kernel, (Z, Y, TP, TC, WC, OC)),
        out_shape=[
            jax.ShapeDtypeStruct((N, M), bf),
            jax.ShapeDtypeStruct((sinks.shape[0], N), f32),
        ],
        in_specs=[vmem] * 3 + [hbm] * 9 + [smem] * 2,
        out_specs=[vmem, vmem],
        scratch_shapes=[pltpu.VMEM(part.shape, bf) for part in weights]
        + [
            pltpu.VMEM((Z, KD, C), bf),
            pltpu.VMEM((Z * N, D), bf),
            pltpu.VMEM((D, C), bf),
            pltpu.VMEM(gates.shape, bf),
            pltpu.VMEM((S * w_out.shape[0], M), bf),
            pltpu.VMEM((Z * N, C + LANES), f32),
            pltpu.VMEM((LANES, N), f32),
            pltpu.VMEM((Z * N, C), bf),
            pltpu.VMEM((Z * N, LANES), f32),
            pltpu.VMEM((S, HD, LANES), f32),
            pltpu.VMEM((Z, HD, LANES), f32),
            pltpu.VMEM((Z + 1, WINDOW, LANES), bf),
            pltpu.VMEM((Z, 8, N), f32),
            pltpu.VMEM((Z, 8, N), f32),
            pltpu.VMEM((Z, piece, LANES), bf),
            pltpu.VMEM((TP, Z, piece, LANES), bf),
            pltpu.VMEM((Z, 8, N), f32),
            pltpu.VMEM((Z, 8, N), f32),
            pltpu.VMEM((N, S * w_out.shape[0]), bf),
            dma((9,)),
            dma((2, Z, WC)), dma((2, Z, WC)), dma((Y - 1, Z, WC)), dma((Y - 1, Z, WC)),
            dma((Z,)), dma((Z,)),
            dma((2, Z, TC)), dma((Z, TC)), dma((XH - 1, Z, TC)), dma((XH - 1, Z, TC)),
            dma((XH, Z, TC)), dma((XH, Z, TC)),
            dma((2, Z, OC)), dma((Z, OC)), dma((Y - 1, Z, OC)), dma((Y - 1, Z, OC)),
            dma((Z,)), dma((Z,)), dma((Y - 1, Z)), dma((Y - 1, Z)),
            dma((Z,)), dma((Z,)), dma((Z,)), dma((Z,)),
            dma((XH - 1, Z)), dma((XH - 1, Z)), dma((XH, Z)), dma((XH, Z)),
        ],
        compiler_params=pltpu.CompilerParams(
            collective_id=0, has_side_effects=True, vmem_limit_bytes=60 * 2**20
        ),
    )(tokens, gain, shifts, gates, w_out, *weights, sinks, bias)


def shards(
    tokens,
    norm_gain,
    w_query,
    w_key,
    w_value,
    w_mem_query,
    w_mem_key,
    w_mem_value,
    w_mem_gate,
    w_gates,
    sinks,
    forget_bias,
    forget_shift,
    w_out,
):
    weights = (w_query, w_key, w_value, w_mem_query, w_mem_key, w_mem_value, w_mem_gate)
    mixed, totals = mix(
        tokens,
        norm_gain[None, :],
        forget_shift.T,
        w_gates.reshape(w_gates.shape[0], -1),
        w_out,
        weights,
        sinks,
        forget_bias,
    )
    return mixed, totals.T


def solution(mesh):
    placed = (
        P(("sp", "tp"), None),
        P(),
        P("sp", "tp"),
        P("sp", "tp"),
        P("sp", "tp"),
        P("sp", "tp"),
        P("sp", "tp"),
        P("sp", "tp"),
        P("sp", "tp"),
        P(),
        P("tp"),
        P("tp"),
        P("sp", "tp"),
        P("sp", "tp"),
    )
    return jax.shard_map(
        shards,
        mesh=mesh,
        in_specs=placed,
        out_specs=(P("sp", "tp"), P("sp", "tp")),
        check_vma=False,
    )
```

```python
import functools
import math

import jax
import jax.numpy as jnp
from jax import lax
from jax.experimental import pallas as pl
from jax.experimental.pallas import tpu as pltpu
from jax.sharding import PartitionSpec as P

HD = 64
WINDOW = 128
LANES = 128
EPSILON = 1e-06
MASKED = -1e30
MESH = pl.DeviceIdType.MESH


def begin(copy):
    copy.start()


def drain(copy):
    copy.wait_send()


def dot(left, right, **more):
    return jnp.dot(left, right, preferred_element_type=jnp.float32, **more)


def lanes_of(shape):
    return lax.broadcasted_iota(jnp.int32, shape, len(shape) - 1)


def mixer_kernel(
    sizes,
    tokens, gain, shifts, gates, w_out, w_query, w_key, w_value, w_mem_query, w_mem_key,
    w_mem_value, w_mem_gate, sinks, bias,
    mixed, totals,
    in_query, in_key, in_value, in_mem_query, in_mem_key, in_mem_value, in_mem_gate,
    PM, PA, T, WM, WA, GW, O, ACC, ACCA, FLAT, PROJ, PROJA, NUM, ST, EB, HALO, SH, FS,
    JSM, JSA, JM, JA, LS, LT, X, MIX,
    own_sems, w_send, w_recv, wa_send, wa_recv, wy_send, wy_recv, wb_send, wb_recv,
    f_send, f_recv, tz_send, tz_recv, tx_send, tx_recv, tt_send, tt_recv,
    oz_send, oz_recv, oy_send, oy_recv, h_send, h_recv, s_send, s_recv,
    jz_send, jz_recv, ja_send, ja_recv, l_send, l_recv,
    jx_send, jx_recv, jt_send, jt_recv, jxa_send, jxa_recv, jta_send, jta_recv,
):
    Z, Y, TP, TC, WC, OC = sizes
    XH = TP // 2
    R, D = tokens.shape
    N = R * TP
    HOLD, KD, CA = PA.shape
    CM = PM.shape[2]
    offset = (Z - HOLD) // 2
    KO, M = w_out.shape
    MC = WC // 2
    RC, RW, RM, RO = R // TC, KD // WC, KD // MC, KO // OC
    S = Z * Y
    sp, tp = lax.axis_index("sp"), lax.axis_index("tp")
    z, y = sp // Y, sp % Y
    twin = tp + 1 - 2 * (tp % 2)

    def is_holder(zz):
        return (zz >= offset) & (zz < offset + HOLD)

    holds = is_holder(z)
    can_up, can_down = z < Z - 1, z > 0

    def remote(src, dst, send, recv, to_sp, to_tp):
        return pltpu.make_async_remote_copy(
            src_ref=src, dst_ref=dst, send_sem=send, recv_sem=recv,
            device_id={"sp": to_sp, "tp": to_tp}, device_id_type=MESH,
        )

    def side_tp(k):
        return (tp + 2 * k) % TP

    def from_tp(k):
        return (tp + TP - 2 * k) % TP

    def up_z(k):
        return (z + k) % Z

    def back_z(k):
        return (z + Z - k) % Z

    def up_y(k):
        return (y + k) % Y

    def back_y(k):
        return (y + Y - k) % Y

    def m_rows(zz, yy, c):
        return WM.at[pl.ds(pl.multiple_of((zz * Y + yy) * KD + c * RM, RM), RM), :]

    def a_rows(zz, yy, c):
        return WA.at[pl.ds(pl.multiple_of((zz * Y + yy) * KD + c * RW, RW), RW), :]

    def m_across(way, d, c, source, piece):
        to = z + d * (1 - 2 * way)
        return remote(
            PM.at[piece, pl.ds(c * RM, RM), :], m_rows(source, y, c),
            w_send.at[way, d, c], w_recv.at[way, d, c], to * Y + y, tp,
        )

    def a_across(way, d, c, source, piece):
        to = z + d * (1 - 2 * way)
        return remote(
            PA.at[piece, pl.ds(c * RW, RW), :], a_rows(source, y, c),
            wa_send.at[way, d, c], wa_recv.at[way, d, c], to * Y + y, tp,
        )

    def m_side(zz, j, c, source):
        place = m_rows(zz, source, c)
        return remote(
            place, place, wy_send.at[j - 1, zz, c], wy_recv.at[j - 1, zz, c], z * Y + up_y(j), tp
        )

    def a_side(zz, j, c, source):
        place = a_rows(zz, source, c)
        return remote(
            place, place, wb_send.at[j - 1, zz, c], wb_recv.at[j - 1, zz, c], z * Y + up_y(j), tp
        )

    def f_across(k, source):
        return remote(
            SH.at[up_z(k)], FS.at[source], f_send.at[k], f_recv.at[k], up_z(k) * Y + y, tp
        )

    def t_rows(zz, tt, c):
        start = pl.multiple_of((zz * TP + tt) * R + c * RC, RC)
        return T.at[pl.ds(start, RC), :]

    def t_line(zz, way, c):
        place = t_rows(zz, tp, c)
        to = (z + 1 - 2 * way) * Y + y
        return remote(place, place, tz_send.at[way, zz, c], tz_recv.at[zz, c], to, tp)

    def t_side(zz, k, c, source):
        place = t_rows(zz, source, c)
        return remote(place, place, tx_send.at[k - 1, zz, c], tx_recv.at[k - 1, zz, c], sp, side_tp(k))

    def t_twin(zz, k, c, source):
        place = t_rows(zz, source, c)
        return remote(place, place, tt_send.at[k, zz, c], tt_recv.at[k, zz, c], sp, twin)

    def o_rows(zz, yy, c):
        start = pl.multiple_of((zz * Y + yy) * KO + c * RO, RO)
        return O.at[pl.ds(start, RO), :]

    def o_line(zz, way, c, own):
        place = o_rows(zz, y, c)
        src = w_out.at[pl.ds(c * RO, RO), :] if own else place
        to = (z + 1 - 2 * way) * Y + y
        return remote(src, place, oz_send.at[way, zz, c], oz_recv.at[zz, c], to, tp)

    def o_side(zz, k, c, source, own):
        place = o_rows(zz, source, c)
        src = w_out.at[pl.ds(c * RO, RO), :] if own else place
        return remote(src, place, oy_send.at[k - 1, zz, c], oy_recv.at[k - 1, zz, c], z * Y + up_y(k), tp)

    def h_side(zz, shift):
        rows = pl.ds(pl.multiple_of(zz * N + N - WINDOW, WINDOW), WINDOW)
        return remote(
            PROJA.at[rows, pl.ds(CA - LANES, LANES)], HALO.at[zz + shift],
            h_send.at[zz], h_recv.at[zz], z * Y + up_y(1), tp,
        )

    def s_side(zz, k, source):
        place = ST.at[zz * Y + source]
        return remote(place, place, s_send.at[k - 1, zz], s_recv.at[k - 1, zz], z * Y + up_y(k), tp)

    def j_across(k, source):
        return remote(
            JSM.at[up_z(k)], JM.at[tp, source], jz_send.at[k], jz_recv.at[k], up_z(k) * Y + y, tp
        )

    def ja_across(k, holder):
        return remote(
            JSA.at[up_z(k)], JA.at[tp, holder], ja_send.at[k], ja_recv.at[k], up_z(k) * Y + y, tp
        )

    def l_across(k, holder):
        return remote(
            LS.at[up_z(k)], LT.at[holder], l_send.at[k], l_recv.at[k], up_z(k) * Y + y, tp
        )

    def j_side(zz, k, source):
        place = JM.at[source, zz]
        return remote(place, place, jx_send.at[k - 1, zz], jx_recv.at[k - 1, zz], sp, side_tp(k))

    def j_twin(zz, k, source):
        place = JM.at[source, zz]
        return remote(place, place, jt_send.at[k, zz], jt_recv.at[k, zz], sp, twin)

    def ja_side(a, k, source):
        place = JA.at[source, a]
        return remote(place, place, jxa_send.at[k - 1, a], jxa_recv.at[k - 1, a], sp, side_tp(k))

    def ja_twin(a, k, source):
        place = JA.at[source, a]
        return remote(place, place, jta_send.at[k, a], jta_recv.at[k, a], sp, twin)

    ins = (
        (w_query, in_query), (w_key, in_key), (w_value, in_value), (w_mem_query, in_mem_query),
        (w_mem_key, in_mem_key), (w_mem_value, in_mem_value), (w_mem_gate, in_mem_gate),
        (w_out, O.at[pl.ds(pl.multiple_of(sp * KO, KO), KO), :]),
    )
    keep = [pltpu.make_async_copy(a, b, own_sems.at[i]) for i, (a, b) in enumerate(ins)]

    barrier = pltpu.get_barrier_semaphore()
    greeted = [(up_z(k) * Y + y, tp) for k in range(1, Z)]
    greeted += [(z * Y + up_y(k), tp) for k in range(1, Y)]
    greeted += [(sp, side_tp(k)) for k in range(1, XH)] + [(sp, twin)]
    for to_sp, to_tp in greeted:
        pl.semaphore_signal(
            barrier, inc=1, device_id={"sp": to_sp, "tp": to_tp}, device_id_type=MESH
        )
    for copy in keep:
        copy.start()

    step = 16
    for i in range(R // step):
        values = tokens[pl.ds(i * step, step), :].astype(jnp.float32)
        rescale = lax.rsqrt(jnp.mean(values * values, axis=-1, keepdims=True) + EPSILON)
        start = pl.multiple_of((z * TP + tp) * R + i * step, step)
        T[pl.ds(start, step), :] = (values * rescale * gain[...]).astype(jnp.bfloat16)
    for i in range(Z):
        SH[i, 0:1, :] = shifts[i : i + 1, :]
    FS[z] = SH[z]

    @pl.when(y == 0)
    def _():
        HALO[0] = jnp.zeros(HALO.shape[1:], HALO.dtype)

    with jax.named_scope('barrier_wait'):
        pl.semaphore_wait(barrier, len(greeted))

    def pack():
        for copy in keep[:7]:
            copy.wait()
        high = min(KD, WINDOW)
        lane = lanes_of((high, LANES))
        qa = CA - LANES

        def halves(rows, left, i, right, j):
            a = left[rows, pl.ds(i // 2 * LANES, LANES)].astype(jnp.float32)
            b = right[rows, pl.ds(j // 2 * LANES, LANES)].astype(jnp.float32)
            a = pltpu.roll(a, HD, 1) if i % 2 else a
            b = b if j % 2 else pltpu.roll(b, HD, 1)
            return jnp.where(lane < HD, a, b).astype(jnp.bfloat16)

        def some(r, nothing):
            rows = pl.ds(pl.multiple_of(r * high, high), high)
            for i in range(Z):
                PM[i, rows, :LANES] = halves(rows, in_mem_query, i, in_mem_key, i)
                PM[i, rows, LANES:] = halves(rows, in_mem_value, i, in_mem_gate, i)
            for i in range(HOLD):
                PA[i, rows, :qa] = in_query[rows, i * qa : (i + 1) * qa]
                PA[i, rows, qa:] = halves(rows, in_key, i, in_value, i)
            return nothing

        lax.fori_loop(0, KD // high, some, 0)
        rows = pl.ds(pl.multiple_of(sp * KD, KD), KD)
        WM[rows, :] = PM[z]

        @pl.when(holds)
        def _():
            WA[rows, :] = PA[z - offset]

    def ways(d):
        return ((0, z + d < Z, z - d >= 0), (1, z - d >= 0, z + d < Z))

    def weights_out(way, d, act):
        to = z + d * (1 - 2 * way)

        @pl.when(is_holder(to))
        def _():
            for c in range(WC):
                act(a_across(way, d, c, z, to - offset))

        for c in range(MC):
            act(m_across(way, d, c, z, to))

    def weights_far(act):
        for d in range(Z - 1, 1, -1):
            for way, there, _ in ways(d):
                pl.when(there)(lambda: weights_out(way, d, act))

    def weights_aside(zz, act):
        for j in range(1, Y):
            for c in range(MC):
                act(m_side(zz, j, c, y))

            @pl.when(holds)
            def _():
                for c in range(WC):
                    act(a_side(zz, j, c, y))

    def weights_on(d, act):
        for way, _, there in ways(d):
            origin = z - d * (1 - 2 * way)

            def landed_a(way=way, origin=origin):
                for c in range(WC):
                    if act is begin:
                        a_across(way, d, c, origin, 0).wait_recv()
                    for j in range(1, Y):
                        act(a_side(origin, j, c, y))

            def landed_m(way=way, origin=origin):
                for c in range(MC):
                    if act is begin:
                        m_across(way, d, c, origin, 0).wait_recv()
                    for j in range(1, Y):
                        act(m_side(origin, j, c, y))

            pl.when(there & holds)(landed_a)
            pl.when(there)(landed_m)

    def own_tokens(act):
        for c in range(TC):
            pl.when(can_up)(lambda: act(t_line(z, 0, c)))
            pl.when(can_down)(lambda: act(t_line(z, 1, c)))
            for k in range(1, XH):
                act(t_side(z, k, c, tp))
            act(t_twin(z, 0, c, tp))

    def tokens_on(d, act):
        for way, origin, there, further in (
            (0, z - d, z - d >= 0, can_up), (1, z + d, z + d < Z, can_down),
        ):
            def landed(way=way, origin=origin, further=further):
                for c in range(TC):
                    if act is begin:
                        t_line(origin, way, c).wait_recv()
                    pl.when(further)(lambda: act(t_line(origin, way, c)))
                    for k in range(1, XH):
                        act(t_side(origin, k, c, tp))
                    act(t_twin(origin, 0, c, tp))

            pl.when(there)(landed)

    def tokens_aside(zz, act):
        for k in range(1, XH):
            for c in range(TC):
                if act is begin:
                    t_side(zz, k, c, from_tp(k)).wait_recv()
                act(t_twin(zz, k, c, from_tp(k)))

    def output_aside(act):
        for c in range(OC):
            for k in range(1, Y):
                act(o_side(z, k, c, y, True))

    def own_output(act):
        for c in range(OC):
            pl.when(can_up)(lambda: act(o_line(z, 0, c, True)))
            pl.when(can_down)(lambda: act(o_line(z, 1, c, True)))

    def output_on(d, act, line=True, aside=True):
        for way, origin, there, further in (
            (0, z - d, z - d >= 0, can_up), (1, z + d, z + d < Z, can_down),
        ):
            def landed(way=way, origin=origin, further=further):
                for c in range(OC):
                    if act is begin and line:
                        o_line(origin, way, c, False).wait_recv()
                    if line:
                        pl.when(further)(lambda: act(o_line(origin, way, c, False)))
                    if aside:
                        for k in range(1, Y):
                            act(o_side(origin, k, c, y, False))

            pl.when(there)(landed)

    def output_pieces(first, last, act):
        for c, way in [(c, way) for c in range(OC) for way in range(2)][first:last]:
            origin = z - 1 + 2 * way

            @pl.when((origin >= 0) & (origin < Z))
            def _():
                for k in range(1, Y):
                    act(o_side(origin, k, c, y, False))

    def block_rows(zz):
        return pl.ds(pl.multiple_of(zz * N, N), N)

    depth = Y * KD

    def project(zk):
        cols = pl.ds(pl.multiple_of(zk * depth, depth), depth)

        def part(b, nothing):
            rows = block_rows(b)
            block = T[rows, cols]
            ACC[rows, :CM] += dot(block, WM[cols, :])
            ACC[rows, CM:] += dot(block, GW[cols, :])

            @pl.when(holds)
            def _():
                ACCA[rows, :] += dot(block, WA[cols, :])

            return nothing

        lax.fori_loop(0, Z, part, 0)

    parts = N // WINDOW
    wide = (WINDOW, LANES)

    def sub_rows(zz, i):
        return pl.ds(pl.multiple_of(zz * N + i * WINDOW, WINDOW), WINDOW)

    def attend(zz, i, before, pair):
        lane = lanes_of(wide)
        heads = PROJA[sub_rows(zz, i), pair * LANES : (pair + 1) * LANES].astype(jnp.float32) * HD ** (-0.5)
        first = jnp.where(lane < HD, heads, 0.0)
        second = jnp.where(lane < HD, pltpu.roll(heads, HD, 1), 0.0)
        query = jnp.concatenate([first, second], axis=0).astype(jnp.bfloat16)
        rows = jnp.concatenate([before, PROJA[sub_rows(zz, i), CA - LANES :]], axis=0)
        scores = lax.dot_general(
            query, rows, (((1,), (1,)), ((), ())), preferred_element_type=jnp.float32
        )
        shape = (2 * WINDOW, 2 * WINDOW)
        at = lax.broadcasted_iota(jnp.int32, shape, 0)
        head = at >= WINDOW
        key_at = lax.broadcasted_iota(jnp.int32, shape, 1)
        distance = jnp.where(head, at - WINDOW, at) - key_at + WINDOW
        allowed = (distance >= 0) & (distance < WINDOW)
        if i == 0:
            lowest = WINDOW * (1 - jnp.minimum(zz * Y + y, 1))
            allowed = allowed & (key_at >= lowest)
        scores = jnp.where(allowed, scores, MASKED)
        tall = lax.broadcasted_iota(jnp.int32, (2 * WINDOW, 1), 0) >= WINDOW
        at_sink = (z - offset) * (CA - LANES) // HD + 2 * pair
        sink = jnp.where(tall, sinks[at_sink + 1], sinks[at_sink])
        ceiling = jnp.maximum(jnp.max(scores, axis=-1, keepdims=True), sink)
        weights = jnp.exp(scores - ceiling)
        total = jnp.exp(sink - ceiling) + jnp.sum(weights, axis=-1, keepdims=True)
        probs = (weights * (1.0 / total)).astype(jnp.bfloat16)
        out = dot(probs, rows)
        both = jnp.where(lane < HD, pltpu.roll(out[:WINDOW], HD, 1), out[WINDOW:])
        JSA[zz, pl.ds(pair * N + i * WINDOW, WINDOW), :] = both.astype(jnp.bfloat16)
        logs = jnp.broadcast_to(ceiling + jnp.log(total), (2 * WINDOW, LANES)).T
        LS[zz, 2 * pair : 2 * pair + 1, pl.ds(i * WINDOW, WINDOW)] = logs[0:1, :WINDOW]
        LS[zz, 2 * pair + 1 : 2 * pair + 2, pl.ds(i * WINDOW, WINDOW)] = logs[0:1, WINDOW:]

    def remember(zz):
        FLAT[...] = ACC[block_rows(zz), CM:].T
        gate_count = gates.shape[0] // 2
        head = tp * Z + z
        log_in = FLAT[pl.ds(head, 1), :] - 0.5 * math.log(N * S)
        pre = FLAT[pl.ds(gate_count + head, 1), :] + bias[z]
        log_sig = jnp.minimum(pre, 0.0) - jnp.log1p(jnp.exp(-jnp.abs(pre)))
        log_forget = log_sig + FS[zz][0:1, :]
        square = (N, N)
        before = lax.broadcasted_iota(jnp.int32, square, 0) <= lax.broadcasted_iota(
            jnp.int32, square, 1
        )
        summed = dot(
            jnp.broadcast_to(log_forget, (8, N)), before.astype(jnp.float32),
            precision=lax.Precision.HIGHEST,
        )[0:1, :]
        passed = summed[:, N - 1 :]
        decays = passed - summed + log_in
        level = jnp.max(decays, axis=1, keepdims=True)
        weights = jnp.exp(decays - level)
        pair = PROJ[block_rows(zz), :LANES].astype(jnp.float32)
        query = (pair[:, :HD] * HD ** (-0.5)).astype(jnp.bfloat16)
        keys = pair.T[HD:, :]
        lane = lanes_of((N, LANES))
        values = PROJ[block_rows(zz), LANES:].astype(jnp.float32)
        values = jnp.where(lane < HD, values, jnp.where(lane == HD, 1.0, 0.0)).astype(jnp.bfloat16)
        state = dot((keys * weights).astype(jnp.bfloat16), values)
        lane = lanes_of(state.shape)
        state = jnp.where(lane == HD + 1, passed, jnp.where(lane == HD + 2, level, state))
        ST[zz * Y + y] = state
        keys = keys.astype(jnp.bfloat16)
        summed_col = jnp.broadcast_to(summed, (LANES, N)).T
        source = log_in - summed
        lane = lanes_of(wide)
        for i in range(parts):
            width = (i + 1) * WINDOW
            span = (WINDOW, width)
            causal = lax.broadcasted_iota(jnp.int32, span, 0) + i * WINDOW >= lanes_of(span)
            since = summed_col[i * WINDOW : (i + 1) * WINDOW, :]
            log_weight = jnp.where(causal, since[:, :1] + source[:, :width], MASKED)
            peak = jnp.max(log_weight, axis=-1, keepdims=True)
            affinity = dot(query[i * WINDOW : (i + 1) * WINDOW], keys[:, :width]) * jnp.exp(
                log_weight - peak
            )
            total = jnp.sum(affinity, axis=-1, keepdims=True)
            found = dot(affinity.astype(jnp.bfloat16), values[:width])
            NUM[sub_rows(zz, i), :] = jnp.where(
                lane < HD, found,
                jnp.where(lane == HD, total, jnp.where(lane == HD + 1, peak, since)),
            )

    def local_work(zz):
        PROJ[block_rows(zz), :] = ACC[block_rows(zz), :CM].astype(jnp.bfloat16)

        @pl.when(holds)
        def _():
            PROJA[block_rows(zz), :] = ACCA[block_rows(zz), :].astype(jnp.bfloat16)

        with jax.named_scope('remember'):
            remember(zz)

        @pl.when(holds)
        def _():
            h_side(zz, (y + 1) // Y).start()
            with jax.named_scope('attend'):
                for i in range(1, parts):
                    before = PROJA[sub_rows(zz, i - 1), CA - LANES :]
                    for pair in range(CA // LANES - 1):
                        attend(zz, i, before, pair)

        for k in range(1, Y):
            s_side(zz, k, y).start()

    def near(d, act):
        pl.when((z == d) & can_up)(lambda: weights_out(0, 1, act))
        pl.when((z == Z - 1 - d) & can_down)(lambda: weights_out(1, 1, act))

    own_tokens(begin)
    with jax.named_scope('pack'):
        pack()
    for k in range(1, Z):
        f_across(k, z).start()
    weights_aside(z, begin)
    output_aside(begin)
    near(0, begin)
    ACC[...] = jnp.zeros_like(ACC)
    ACCA[...] = jnp.zeros_like(ACCA)

    def turn(i, nothing):
        cols = pl.ds(pl.multiple_of(i * LANES, LANES), LANES)
        count = gates.shape[0]
        tall = jnp.concatenate(
            [gates[:, cols].astype(jnp.float32), jnp.zeros((LANES - count, LANES), jnp.float32)],
            axis=0,
        )
        GW[cols, :] = tall.T.astype(jnp.bfloat16)
        return nothing

    lax.fori_loop(0, D // LANES, turn, 0)

    def both_sides(d, act):
        def one(side, nothing):
            zz = z + d * (2 * side - 1)
            pl.when((zz >= 0) & (zz < Z) & (d + 1 - side > 0))(lambda: act(zz))
            return nothing

        lax.fori_loop(0, 2, one, 0)

    def stage(d, nothing):
        with jax.named_scope('t_on'):
            tokens_on(d, begin)
        near(d, begin)

        inside = can_up & can_down

        @pl.when((d == Z - 1) & jnp.logical_not(inside))
        def _():
            weights_far(begin)

        @pl.when((d == Z - 1) & inside)
        def _():
            weights_far(begin)

        pl.when(d == Z - 1)(lambda: own_output(begin))

        @pl.when((d == 2) & inside)
        def _():
            with jax.named_scope('w_on_mid'):
                weights_on(1, begin)

        with jax.named_scope('t_aside'):
            both_sides(d - 1, lambda zz: tokens_aside(zz, begin))
        return nothing

    lax.fori_loop(1, Z, stage, 0)
    with jax.named_scope('w_on_3'):
        for d in range(Z - 1, 2, -1):
            weights_on(d, begin)
    with jax.named_scope('t_last'):
        both_sides(Z - 1, lambda zz: tokens_aside(zz, begin))
        for zz in range(Z):
            for k in range(XH):
                for c in range(TC):
                    t_twin(zz, k, c, (twin + TP - 2 * k) % TP).wait_recv()

    def multiply(zz):
        with jax.named_scope('w_side'):
            for j in range(1, Y):
                for c in range(MC):
                    m_side(zz, j, c, back_y(j)).wait_recv()

                @pl.when(holds)
                def _():
                    for c in range(WC):
                        a_side(zz, j, c, back_y(j)).wait_recv()

        with jax.named_scope('project'):
            project(zz)

    both_sides(0, multiply)

    @pl.when(jnp.logical_not(can_up & can_down))
    def _():
        with jax.named_scope('w_on_1'):
            weights_on(1, begin)

    for d in range(Z - 1, 2, -1):
        both_sides(d, multiply)
    if Z > 2:
        with jax.named_scope('w_on_2'):
            weights_on(2, begin)
    for d in range(1, min(Z, 3)):
        both_sides(d, multiply)
    for k in range(1, Z):
        f_across(k, back_z(k)).wait_recv()

    with jax.named_scope('o_line_1'):
        output_on(1, begin, aside=False)

    def local(zz, nothing):
        local_work(zz)
        for i in range(4):
            pl.when(zz == i)(lambda: output_pieces(i, 1 + i, begin))
        return nothing

    lax.fori_loop(0, Z, local, 0)

    output_pieces(4, 2 * OC, begin)

    with jax.named_scope('halo_state'):
        for zz in range(Z):
            pl.when(holds)(lambda: h_side(zz, 1 - jnp.minimum(y, 1)).wait_recv())
            for k in range(1, Y):
                s_side(zz, k, back_y(k)).wait_recv()

    def enter():
        carried = jnp.zeros((HD, LANES), jnp.float32)
        stabilizer = jnp.full((1, 1), MASKED, jnp.float32)
        lane = lanes_of((HD, LANES))
        for i in range(S):
            @pl.when(y == i % Y)
            def _(carried=carried, stabilizer=stabilizer):
                EB[i // Y] = jnp.where(lane == HD + 1, stabilizer, carried)

            state = ST[i]
            passed, level = state[0:1, HD + 1 : HD + 2], state[0:1, HD + 2 : HD + 3]
            newer = jnp.maximum(stabilizer + passed, level)
            carried = carried * jnp.exp(stabilizer + passed - newer) + state * jnp.exp(level - newer)
            stabilizer = newer

    enter()

    def finish(zz):
        @pl.when(holds)
        def _():
            for pair in range(CA // LANES - 1):
                attend(zz, 0, HALO[zz], pair)

        entering = EB[zz]
        stabilizer = entering[0:1, HD + 1 : HD + 2]
        local = NUM[block_rows(zz), :]
        peak, since = local[:, HD + 1 : HD + 2], local[:, HD + 2 : HD + 3]
        pair = PROJ[block_rows(zz), :LANES].astype(jnp.float32)
        query = (pair[:, :HD] * HD ** (-0.5)).astype(jnp.bfloat16)
        carried = dot(query, entering.astype(jnp.bfloat16))
        older = since + stabilizer
        row_level = jnp.maximum(older, peak)
        found = jnp.exp(older - row_level) * carried + jnp.exp(peak - row_level) * local
        bound = jnp.maximum(jnp.abs(found[:, HD : HD + 1]), jnp.exp(-row_level))
        gate = pltpu.roll(
            PROJ[block_rows(zz), LANES:].astype(jnp.float32), HD, 1
        )
        recall = found / bound * jax.nn.sigmoid(gate)
        half = N // 2
        lane = lanes_of((half, LANES))
        paired = jnp.where(lane < HD, recall[:half], pltpu.roll(recall[half:], HD, 1))
        JSM[zz] = paired.astype(jnp.bfloat16)

    def hand_over(k, act):
        act(j_across(k, z))

        @pl.when(holds)
        def _():
            act(ja_across(k, z - offset))
            act(l_across(k, z - offset))

    for k in range(1, Z):
        with jax.named_scope('finish'):
            finish(up_z(k))
        hand_over(k, begin)
    with jax.named_scope('finish'):
        finish(z)
    JM[tp, z] = JSM[z]

    @pl.when(holds)
    def _():
        JA[tp, z - offset] = JSA[z]
        LT[z - offset] = LS[z]

    def share(k, act):
        zz = back_z(k)
        if k and act is begin:
            j_across(k, zz).wait_recv()
        for j in range(1, XH):
            act(j_side(zz, j, tp))
        act(j_twin(zz, 0, tp))

        @pl.when(is_holder(zz))
        def _():
            if k and act is begin:
                ja_across(k, zz - offset).wait_recv()
            for j in range(1, XH):
                act(ja_side(zz - offset, j, tp))
            act(ja_twin(zz - offset, 0, tp))

    def share_aside(act):
        for zz in range(Z):
            for j in range(1, XH):
                if act is begin:
                    j_side(zz, j, from_tp(j)).wait_recv()
                act(j_twin(zz, j, from_tp(j)))
        for a in range(HOLD):
            for j in range(1, XH):
                if act is begin:
                    ja_side(a, j, from_tp(j)).wait_recv()
                act(ja_twin(a, j, from_tp(j)))

    share(0, begin)
    for d in range(2, Z):
        with jax.named_scope('o_on_2'):
            output_on(d, begin)
        if d == 2:
            with jax.named_scope('share'):
                for k in range(1, Z):
                    share(k, begin)
            with jax.named_scope('share_aside'):
                share_aside(begin)
    with jax.named_scope('share_wait'):
        for k in range(1, Z):
            origin = back_z(k)
            pl.when(is_holder(origin))(lambda: l_across(k, origin - offset).wait_recv())
        for k in range(XH):
            for zz in range(Z):
                j_twin(zz, k, (twin + TP - 2 * k) % TP).wait_recv()
            for a in range(HOLD):
                ja_twin(a, k, (twin + TP - 2 * k) % TP).wait_recv()

    mem_base = TP * sinks.shape[0] * HD
    per_tp = sinks.shape[0] * HD
    half = N // 2
    pairs = CA // LANES - 1
    for t in range(TP):
        for a in range(HOLD):
            for pair in range(pairs):
                at = t * per_tp + (a * pairs + pair) * LANES
                X[:, at : at + LANES] = JA[t, a, pair * N : (pair + 1) * N, :]
        for zz in range(Z):
            at = mem_base + (t * Z + zz) * HD
            X[:half, at : at + HD] = JM[t, zz, :, :HD]
            X[half:, at : at + HD] = JM[t, zz, :, HD:]
    for a in range(HOLD):
        totals[2 * pairs * a : 2 * pairs * (a + 1), :] = LT[a, : 2 * pairs, :]

    tile = min(256, M)
    deep = Y * KO

    def outputs(zz):
        for k in range(1, Y):
            for c in range(OC):
                o_side(zz, k, c, back_y(k), False).wait_recv()
        part = pl.ds(pl.multiple_of(zz * deep, deep), deep)

        def columns(i, nothing):
            cols = pl.ds(pl.multiple_of(i * tile, tile), tile)
            MIX[:, cols] += dot(X[:, part], O[part, cols])
            return nothing

        lax.fori_loop(0, M // tile, columns, 0)

    MIX[...] = jnp.zeros_like(MIX)
    keep[7].wait()

    def stage_three(d, nothing):
        with jax.named_scope('outputs'):
            both_sides(d, outputs)
        return nothing

    lax.fori_loop(0, Z, stage_three, 0)
    mixed[...] = MIX[...].astype(jnp.bfloat16)

    own_tokens(drain)
    weights_far(drain)
    weights_aside(z, drain)
    output_aside(drain)
    own_output(drain)
    for k in range(1, Z):
        f_across(k, z).wait_send()

    def settle(i, nothing):
        weights_on(i, drain)
        tokens_on(i, drain)
        output_on(i, drain)
        return nothing

    for d in range(Z):
        near(d, drain)
    lax.fori_loop(1, Z, settle, 0)
    for zz in range(Z):
        tokens_aside(zz, drain)
        pl.when(holds)(lambda: h_side(zz, (y + 1) // Y).wait_send())
        for k in range(1, Y):
            s_side(zz, k, y).wait_send()
    for k in range(1, Z):
        hand_over(k, drain)
    for k in range(Z):
        share(k, drain)
    share_aside(drain)


def mix(tokens, gain, shifts, gates, w_out, weights, sinks, bias):
    S, TP = lax.axis_size("sp"), lax.axis_size("tp")
    Z = shifts.shape[0]
    Y, XH = S // Z, TP // 2
    R, D = tokens.shape
    N = R * TP
    KD = weights[0].shape[0]
    HOLD = weights[1].shape[1] // HD
    CA = weights[0].shape[1] // HOLD + 2 * HD
    CM = sum(part.shape[1] for part in weights[3:]) // Z
    MC = 2
    TC, OC = 3, 6
    WC = 4
    M = w_out.shape[1]
    bf, f32 = jnp.bfloat16, jnp.float32
    dma = pltpu.SemaphoreType.DMA
    vmem = pl.BlockSpec(memory_space=pltpu.VMEM)
    smem = pl.BlockSpec(memory_space=pltpu.SMEM)
    hbm = pl.BlockSpec(memory_space=pl.ANY)
    return pl.pallas_call(
        functools.partial(mixer_kernel, (Z, Y, TP, TC, WC, OC)),
        out_shape=[
            jax.ShapeDtypeStruct((N, M), bf),
            jax.ShapeDtypeStruct((sinks.shape[0], N), f32),
        ],
        in_specs=[vmem] * 4 + [hbm] * 8 + [smem] * 2,
        out_specs=[vmem] * 2,
        scratch_shapes=[pltpu.VMEM(part.shape, bf) for part in weights]
        + [
            pltpu.VMEM((Z, KD, CM), bf),
            pltpu.VMEM((HOLD, KD, CA), bf),
            pltpu.VMEM((Z * N, D), bf),
            pltpu.VMEM((D, CM), bf),
            pltpu.VMEM((D, CA), bf),
            pltpu.VMEM((D, LANES), bf),
            pltpu.VMEM((S * w_out.shape[0], M), bf),
            pltpu.VMEM((Z * N, CM + LANES), f32),
            pltpu.VMEM((Z * N, CA), f32),
            pltpu.VMEM((LANES, N), f32),
            pltpu.VMEM((Z * N, CM), bf),
            pltpu.VMEM((Z * N, CA), bf),
            pltpu.VMEM((Z * N, LANES), f32),
            pltpu.VMEM((S, HD, LANES), f32),
            pltpu.VMEM((Z, HD, LANES), f32),
            pltpu.VMEM((Z + 1, WINDOW, LANES), bf),
            pltpu.VMEM((Z, 8, N), f32),
            pltpu.VMEM((Z, 8, N), f32),
            pltpu.VMEM((Z, N // 2, LANES), bf),
            pltpu.VMEM((Z, N * (CA // LANES - 1), LANES), bf),
            pltpu.VMEM((TP, Z, N // 2, LANES), bf),
            pltpu.VMEM((TP, HOLD, N * (CA // LANES - 1), LANES), bf),
            pltpu.VMEM((Z, 8, N), f32),
            pltpu.VMEM((HOLD, 8, N), f32),
            pltpu.VMEM((N, S * w_out.shape[0]), bf),
            pltpu.VMEM((N, M), f32),
            dma((8,)),
            dma((2, Z, MC)), dma((2, Z, MC)), dma((2, Z, WC)), dma((2, Z, WC)),
            dma((Y - 1, Z, MC)), dma((Y - 1, Z, MC)), dma((Y - 1, Z, WC)), dma((Y - 1, Z, WC)),
            dma((Z,)), dma((Z,)),
            dma((2, Z, TC)), dma((Z, TC)), dma((XH - 1, Z, TC)), dma((XH - 1, Z, TC)),
            dma((XH, Z, TC)), dma((XH, Z, TC)),
            dma((2, Z, OC)), dma((Z, OC)), dma((Y - 1, Z, OC)), dma((Y - 1, Z, OC)),
            dma((Z,)), dma((Z,)), dma((Y - 1, Z)), dma((Y - 1, Z)),
            dma((Z,)), dma((Z,)), dma((Z,)), dma((Z,)), dma((Z,)), dma((Z,)),
            dma((XH - 1, Z)), dma((XH - 1, Z)), dma((XH, Z)), dma((XH, Z)),
            dma((XH - 1, HOLD)), dma((XH - 1, HOLD)), dma((XH, HOLD)), dma((XH, HOLD)),
        ],
        compiler_params=pltpu.CompilerParams(
            collective_id=0, has_side_effects=True, vmem_limit_bytes=60 * 2**20
        ),
    )(tokens, gain, shifts, gates, w_out, *weights, sinks, bias)


def shards(
    tokens,
    norm_gain,
    w_query,
    w_key,
    w_value,
    w_mem_query,
    w_mem_key,
    w_mem_value,
    w_mem_gate,
    w_gates,
    sinks,
    forget_bias,
    forget_shift,
    w_out,
):
    weights = (w_query, w_key, w_value, w_mem_query, w_mem_key, w_mem_value, w_mem_gate)
    mixed, totals = mix(
        tokens,
        norm_gain[None, :],
        forget_shift.T,
        w_gates.transpose(1, 2, 0).reshape(-1, w_gates.shape[0]),
        w_out,
        weights,
        sinks,
        forget_bias,
    )
    return mixed, totals.T


def solution(mesh):
    placed = (
        P(("sp", "tp"), None),
        P(),
        P("sp", "tp"),
        P("sp", "tp"),
        P("sp", "tp"),
        P("sp", "tp"),
        P("sp", "tp"),
        P("sp", "tp"),
        P("sp", "tp"),
        P(),
        P("tp"),
        P("tp"),
        P("sp", "tp"),
        P("sp", "tp"),
    )
    return jax.shard_map(
        shards,
        mesh=mesh,
        in_specs=placed,
        out_specs=(P("sp", "tp"), P("sp", "tp")),
        check_vma=False,
    )
```

```python
import functools
import math

import jax
import jax.numpy as jnp
from jax import lax
from jax.experimental import pallas as pl
from jax.experimental.pallas import tpu as pltpu
from jax.sharding import PartitionSpec as P

HD = 64
WINDOW = 128
LANES = 128
EPSILON = 1e-06
MASKED = -1e30
MESH = pl.DeviceIdType.MESH


def begin(copy):
    copy.start()


def drain(copy):
    copy.wait_send()


def each(count, act):
    return range(count) if act is begin else (None,)


def dot(left, right, **more):
    return jnp.dot(left, right, preferred_element_type=jnp.float32, **more)


def lanes_of(shape):
    return lax.broadcasted_iota(jnp.int32, shape, len(shape) - 1)


def mixer_kernel(
    sizes,
    tokens, gain, shifts, gates, w_out, w_query, w_key, w_value, w_mem_query, w_mem_key,
    w_mem_value, w_mem_gate, sinks, bias,
    mixed, totals,
    in_query, in_key, in_value, in_mem_query, in_mem_key, in_mem_value, in_mem_gate,
    PM, PA, T, WM, WA, GW, O, ACC, ACCA, FLAT, PROJ, PROJA, NUM, ST, EB, HALO, SH, FS,
    JSM, JSA, JM, JA, LS, LT, X, MIX,
    own_sems, w_send, w_recv, wa_send, wa_recv, wy_send, wy_recv, wb_send, wb_recv,
    f_send, f_recv, tz_send, tz_recv, tx_send, tx_recv, tt_send, tt_recv,
    oz_send, oz_recv, oy_send, oy_recv, h_send, h_recv, s_send, s_recv,
    jz_send, jz_recv, ja_send, ja_recv, l_send, l_recv,
    jx_send, jx_recv, jt_send, jt_recv, jxa_send, jxa_recv, jta_send, jta_recv,
):
    Z, Y, TP, TC, WC, OC = sizes
    XH = TP // 2
    R, D = tokens.shape
    N = R * TP
    HOLD, KD, CA = PA.shape
    CM = PM.shape[2]
    offset = (Z - HOLD) // 2
    KO, M = w_out.shape
    MC = WC // 2
    RC, RW, RM, RO = R // TC, KD // WC, KD // MC, KO // OC
    S = Z * Y
    sp, tp = lax.axis_index("sp"), lax.axis_index("tp")
    z, y = sp // Y, sp % Y
    twin = tp + 1 - 2 * (tp % 2)

    def is_holder(zz):
        return (zz >= offset) & (zz < offset + HOLD)

    holds = is_holder(z)
    can_up, can_down = z < Z - 1, z > 0

    def remote(src, dst, send, recv, to_sp, to_tp):
        return pltpu.make_async_remote_copy(
            src_ref=src, dst_ref=dst, send_sem=send, recv_sem=recv,
            device_id={"sp": to_sp, "tp": to_tp}, device_id_type=MESH,
        )

    def span(base, c, count, size):
        if c is None:
            return pl.ds(pl.multiple_of(base, size), count * size)
        return pl.ds(pl.multiple_of(base + c * size, size), size)

    def slot(c):
        return 0 if c is None else c

    def side_tp(k):
        return (tp + 2 * k) % TP

    def from_tp(k):
        return (tp + TP - 2 * k) % TP

    def up_z(k):
        return (z + k) % Z

    def back_z(k):
        return (z + Z - k) % Z

    def up_y(k):
        return (y + k) % Y

    def back_y(k):
        return (y + Y - k) % Y

    def m_rows(zz, yy, c):
        return WM.at[span((zz * Y + yy) * KD, c, MC, RM), :]

    def a_rows(zz, yy, c):
        return WA.at[span((zz * Y + yy) * KD, c, WC, RW), :]

    def m_across(way, d, c, source, piece):
        to = z + d * (1 - 2 * way)
        return remote(
            PM.at[piece, span(0, c, MC, RM), :], m_rows(source, y, c),
            w_send.at[to], w_recv.at[source, slot(c)], to * Y + y, tp,
        )

    def a_across(way, d, c, source, piece):
        to = z + d * (1 - 2 * way)
        return remote(
            PA.at[piece, span(0, c, WC, RW), :], a_rows(source, y, c),
            wa_send.at[to], wa_recv.at[source, slot(c)], to * Y + y, tp,
        )

    def m_side(zz, j, c, source):
        place = m_rows(zz, source, c)
        return remote(
            place, place, wy_send.at[j - 1, zz], wy_recv.at[j - 1, zz, slot(c)], z * Y + up_y(j), tp
        )

    def a_side(zz, j, c, source):
        place = a_rows(zz, source, c)
        return remote(
            place, place, wb_send.at[j - 1, zz], wb_recv.at[j - 1, zz, slot(c)], z * Y + up_y(j), tp
        )

    def f_across(k, source):
        return remote(
            SH.at[up_z(k)], FS.at[source], f_send.at[k], f_recv.at[k], up_z(k) * Y + y, tp
        )

    def t_rows(zz, tt, c):
        return T.at[span((zz * TP + tt) * R, c, TC, RC), :]

    def t_line(zz, way, c):
        place = t_rows(zz, tp, c)
        to = (z + 1 - 2 * way) * Y + y
        return remote(place, place, tz_send.at[way, zz], tz_recv.at[zz, slot(c)], to, tp)

    def t_side(zz, k, c, source):
        place = t_rows(zz, source, c)
        return remote(place, place, tx_send.at[k - 1, zz], tx_recv.at[k - 1, zz, slot(c)], sp, side_tp(k))

    def t_twin(zz, k, c, source):
        place = t_rows(zz, source, c)
        return remote(place, place, tt_send.at[k, zz], tt_recv.at[k, zz, slot(c)], sp, twin)

    def o_rows(zz, yy, c):
        return O.at[span((zz * Y + yy) * KO, c, OC, RO), :]

    def o_line(zz, way, c, own):
        place = o_rows(zz, y, c)
        src = w_out.at[span(0, c, OC, RO), :] if own else place
        to = (z + 1 - 2 * way) * Y + y
        return remote(src, place, oz_send.at[way, zz], oz_recv.at[zz, slot(c)], to, tp)

    def o_side(zz, k, c, source, own):
        place = o_rows(zz, source, c)
        src = w_out.at[span(0, c, OC, RO), :] if own else place
        return remote(src, place, oy_send.at[k - 1, zz], oy_recv.at[k - 1, zz, slot(c)], z * Y + up_y(k), tp)

    def h_side(zz, shift):
        rows = pl.ds(pl.multiple_of(zz * N + N - WINDOW, WINDOW), WINDOW)
        return remote(
            PROJA.at[rows, pl.ds(CA - LANES, LANES)], HALO.at[zz + shift],
            h_send.at[zz], h_recv.at[zz], z * Y + up_y(1), tp,
        )

    def s_side(zz, k, source):
        place = ST.at[zz * Y + source]
        return remote(place, place, s_send.at[k - 1, zz], s_recv.at[k - 1, zz], z * Y + up_y(k), tp)

    def j_across(k, source):
        return remote(
            JSM.at[up_z(k)], JM.at[tp, source], jz_send.at[k], jz_recv.at[k], up_z(k) * Y + y, tp
        )

    def ja_across(k, holder):
        return remote(
            JSA.at[up_z(k)], JA.at[tp, holder], ja_send.at[k], ja_recv.at[k], up_z(k) * Y + y, tp
        )

    def l_across(k, holder):
        return remote(
            LS.at[up_z(k)], LT.at[holder], l_send.at[k], l_recv.at[k], up_z(k) * Y + y, tp
        )

    def j_side(zz, k, source):
        place = JM.at[source, zz]
        return remote(place, place, jx_send.at[k - 1, zz], jx_recv.at[k - 1, zz], sp, side_tp(k))

    def j_twin(zz, k, source):
        place = JM.at[source, zz]
        return remote(place, place, jt_send.at[k, zz], jt_recv.at[k, zz], sp, twin)

    def ja_side(a, k, source):
        place = JA.at[source, a]
        return remote(place, place, jxa_send.at[k - 1, a], jxa_recv.at[k - 1, a], sp, side_tp(k))

    def ja_twin(a, k, source):
        place = JA.at[source, a]
        return remote(place, place, jta_send.at[k, a], jta_recv.at[k, a], sp, twin)

    ins = (
        (w_query, in_query), (w_key, in_key), (w_value, in_value), (w_mem_query, in_mem_query),
        (w_mem_key, in_mem_key), (w_mem_value, in_mem_value), (w_mem_gate, in_mem_gate),
        (w_out, O.at[pl.ds(pl.multiple_of(sp * KO, KO), KO), :]),
    )
    keep = [pltpu.make_async_copy(a, b, own_sems.at[i]) for i, (a, b) in enumerate(ins)]

    barrier = pltpu.get_barrier_semaphore()
    greeted = [(up_z(k) * Y + y, tp) for k in range(1, Z)]
    greeted += [(z * Y + up_y(k), tp) for k in range(1, Y)]
    greeted += [(sp, side_tp(k)) for k in range(1, XH)] + [(sp, twin)]
    for to_sp, to_tp in greeted:
        pl.semaphore_signal(
            barrier, inc=1, device_id={"sp": to_sp, "tp": to_tp}, device_id_type=MESH
        )
    for copy in keep:
        copy.start()

    step = 16
    for i in range(R // step):
        values = tokens[pl.ds(i * step, step), :].astype(jnp.float32)
        rescale = lax.rsqrt(jnp.mean(values * values, axis=-1, keepdims=True) + EPSILON)
        start = pl.multiple_of((z * TP + tp) * R + i * step, step)
        T[pl.ds(start, step), :] = (values * rescale * gain[...]).astype(jnp.bfloat16)
    for i in range(Z):
        SH[i, 0:1, :] = shifts[i : i + 1, :]
    FS[z] = SH[z]

    @pl.when(y == 0)
    def _():
        HALO[0] = jnp.zeros(HALO.shape[1:], HALO.dtype)

    with jax.named_scope('barrier_wait'):
        pl.semaphore_wait(barrier, len(greeted))

    def pack():
        for copy in keep[:7]:
            copy.wait()
        high = min(KD, WINDOW)
        lane = lanes_of((high, LANES))
        qa = CA - LANES

        def halves(rows, left, i, right, j):
            a = left[rows, pl.ds(i // 2 * LANES, LANES)].astype(jnp.float32)
            b = right[rows, pl.ds(j // 2 * LANES, LANES)].astype(jnp.float32)
            a = pltpu.roll(a, HD, 1) if i % 2 else a
            b = b if j % 2 else pltpu.roll(b, HD, 1)
            return jnp.where(lane < HD, a, b).astype(jnp.bfloat16)

        def some(r, nothing):
            rows = pl.ds(pl.multiple_of(r * high, high), high)
            for i in range(Z):
                PM[i, rows, :LANES] = halves(rows, in_mem_query, i, in_mem_key, i)
                PM[i, rows, LANES:] = halves(rows, in_mem_value, i, in_mem_gate, i)
            for i in range(HOLD):
                PA[i, rows, :qa] = in_query[rows, i * qa : (i + 1) * qa]
                PA[i, rows, qa:] = halves(rows, in_key, i, in_value, i)
            return nothing

        lax.fori_loop(0, KD // high, some, 0)
        rows = pl.ds(pl.multiple_of(sp * KD, KD), KD)
        WM[rows, :] = PM[z]

        @pl.when(holds)
        def _():
            WA[rows, :] = PA[z - offset]

    def ways(d):
        return ((0, z + d < Z, z - d >= 0), (1, z - d >= 0, z + d < Z))

    def weights_out(way, d, act):
        to = z + d * (1 - 2 * way)

        @pl.when(is_holder(to))
        def _():
            for c in each(WC, act):
                act(a_across(way, d, c, z, to - offset))

        for c in each(MC, act):
            act(m_across(way, d, c, z, to))

    def weights_far(act):
        for d in range(Z - 1, 1, -1):
            for way, there, _ in ways(d):
                pl.when(there)(lambda: weights_out(way, d, act))

    def weights_aside(zz, act):
        for j in range(1, Y):
            for c in each(MC, act):
                act(m_side(zz, j, c, y))

            @pl.when(holds)
            def _():
                for c in each(WC, act):
                    act(a_side(zz, j, c, y))

    def weights_on(d, act):
        for way, _, there in ways(d):
            origin = z - d * (1 - 2 * way)

            def landed_a(way=way, origin=origin):
                for c in each(WC, act):
                    if act is begin:
                        a_across(way, d, c, origin, 0).wait_recv()
                    for j in range(1, Y):
                        act(a_side(origin, j, c, y))

            def landed_m(way=way, origin=origin):
                for c in each(MC, act):
                    if act is begin:
                        m_across(way, d, c, origin, 0).wait_recv()
                    for j in range(1, Y):
                        act(m_side(origin, j, c, y))

            pl.when(there & holds)(landed_a)
            pl.when(there)(landed_m)

    def own_tokens(act):
        for c in each(TC, act):
            pl.when(can_up)(lambda: act(t_line(z, 0, c)))
            pl.when(can_down)(lambda: act(t_line(z, 1, c)))
            for k in range(1, XH):
                act(t_side(z, k, c, tp))
            act(t_twin(z, 0, c, tp))

    def tokens_on(d, act, some=None):
        for way, origin, there, further in (
            (0, z - d, z - d >= 0, can_up), (1, z + d, z + d < Z, can_down),
        ):
            def landed(way=way, origin=origin, further=further):
                for c in each(TC, act) if some is None else some:
                    if act is begin:
                        t_line(origin, way, c).wait_recv()
                    pl.when(further)(lambda: act(t_line(origin, way, c)))
                    for k in range(1, XH):
                        act(t_side(origin, k, c, tp))
                    act(t_twin(origin, 0, c, tp))

            pl.when(there)(landed)

    def tokens_aside(zz, act):
        for k in range(1, XH):
            for c in each(TC, act):
                if act is begin:
                    t_side(zz, k, c, from_tp(k)).wait_recv()
                act(t_twin(zz, k, c, from_tp(k)))

    def output_aside(act):
        for c in each(OC, act):
            for k in range(1, Y):
                act(o_side(z, k, c, y, True))

    def own_output(act):
        for c in each(OC, act):
            pl.when(can_up)(lambda: act(o_line(z, 0, c, True)))
            pl.when(can_down)(lambda: act(o_line(z, 1, c, True)))

    def output_on(d, act, line=True, aside=True):
        for way, origin, there, further in (
            (0, z - d, z - d >= 0, can_up), (1, z + d, z + d < Z, can_down),
        ):
            def landed(way=way, origin=origin, further=further):
                for c in each(OC, act):
                    if act is begin and line:
                        o_line(origin, way, c, False).wait_recv()
                    if line:
                        pl.when(further)(lambda: act(o_line(origin, way, c, False)))
                    if aside:
                        for k in range(1, Y):
                            act(o_side(origin, k, c, y, False))

            pl.when(there)(landed)

    def output_pieces(first, last, act):
        for c, way in [(c, way) for c in range(OC) for way in range(2)][first:last]:
            origin = z - 1 + 2 * way

            @pl.when((origin >= 0) & (origin < Z))
            def _():
                for k in range(1, Y):
                    act(o_side(origin, k, c, y, False))

    def block_rows(zz):
        return pl.ds(pl.multiple_of(zz * N, N), N)

    depth = Y * KD

    def project(zk, b):
        cols = pl.ds(pl.multiple_of(zk * depth, depth), depth)

        rows = block_rows(b)
        block = T[rows, cols]
        ACC[rows, :CM] += dot(block, WM[cols, :])
        ACC[rows, CM:] += dot(block, GW[cols, :])

        @pl.when(holds)
        def _():
            ACCA[rows, :] += dot(block, WA[cols, :])

    def project_all(zk):
        def part(b, nothing):
            project(zk, b)
            return nothing

        lax.fori_loop(0, Z, part, 0)

    parts = N // WINDOW
    wide = (WINDOW, LANES)

    def sub_rows(zz, i):
        return pl.ds(pl.multiple_of(zz * N + i * WINDOW, WINDOW), WINDOW)

    def attend(zz, i, before, pair):
        lane = lanes_of(wide)
        heads = PROJA[sub_rows(zz, i), pair * LANES : (pair + 1) * LANES].astype(jnp.float32) * HD ** (-0.5)
        first = jnp.where(lane < HD, heads, 0.0)
        second = jnp.where(lane < HD, pltpu.roll(heads, HD, 1), 0.0)
        query = jnp.concatenate([first, second], axis=0).astype(jnp.bfloat16)
        rows = jnp.concatenate([before, PROJA[sub_rows(zz, i), CA - LANES :]], axis=0)
        scores = lax.dot_general(
            query, rows, (((1,), (1,)), ((), ())), preferred_element_type=jnp.float32
        )
        shape = (2 * WINDOW, 2 * WINDOW)
        at = lax.broadcasted_iota(jnp.int32, shape, 0)
        head = at >= WINDOW
        key_at = lax.broadcasted_iota(jnp.int32, shape, 1)
        distance = jnp.where(head, at - WINDOW, at) - key_at + WINDOW
        allowed = (distance >= 0) & (distance < WINDOW)
        if i == 0:
            lowest = WINDOW * (1 - jnp.minimum(zz * Y + y, 1))
            allowed = allowed & (key_at >= lowest)
        scores = jnp.where(allowed, scores, MASKED)
        tall = lax.broadcasted_iota(jnp.int32, (2 * WINDOW, 1), 0) >= WINDOW
        at_sink = (z - offset) * (CA - LANES) // HD + 2 * pair
        sink = jnp.where(tall, sinks[at_sink + 1], sinks[at_sink])
        ceiling = jnp.maximum(jnp.max(scores, axis=-1, keepdims=True), sink)
        weights = jnp.exp(scores - ceiling)
        total = jnp.exp(sink - ceiling) + jnp.sum(weights, axis=-1, keepdims=True)
        probs = (weights * (1.0 / total)).astype(jnp.bfloat16)
        out = dot(probs, rows)
        both = jnp.where(lane < HD, pltpu.roll(out[:WINDOW], HD, 1), out[WINDOW:])
        JSA[zz, pl.ds(pair * N + i * WINDOW, WINDOW), :] = both.astype(jnp.bfloat16)
        logs = jnp.broadcast_to(ceiling + jnp.log(total), (2 * WINDOW, LANES)).T
        LS[zz, 2 * pair : 2 * pair + 1, pl.ds(i * WINDOW, WINDOW)] = logs[0:1, :WINDOW]
        LS[zz, 2 * pair + 1 : 2 * pair + 2, pl.ds(i * WINDOW, WINDOW)] = logs[0:1, WINDOW:]

    def remember(zz):
        FLAT[...] = ACC[block_rows(zz), CM:].T
        gate_count = gates.shape[0] // 2
        head = tp * Z + z
        log_in = FLAT[pl.ds(head, 1), :] - 0.5 * math.log(N * S)
        pre = FLAT[pl.ds(gate_count + head, 1), :] + bias[z]
        log_sig = jnp.minimum(pre, 0.0) - jnp.log1p(jnp.exp(-jnp.abs(pre)))
        log_forget = log_sig + FS[zz][0:1, :]
        square = (N, N)
        before = lax.broadcasted_iota(jnp.int32, square, 0) <= lax.broadcasted_iota(
            jnp.int32, square, 1
        )
        summed = dot(
            jnp.broadcast_to(log_forget, (8, N)), before.astype(jnp.float32),
            precision=lax.Precision.HIGHEST,
        )[0:1, :]
        passed = summed[:, N - 1 :]
        decays = passed - summed + log_in
        level = jnp.max(decays, axis=1, keepdims=True)
        weights = jnp.exp(decays - level)
        pair = PROJ[block_rows(zz), :LANES].astype(jnp.float32)
        query = (pair[:, :HD] * HD ** (-0.5)).astype(jnp.bfloat16)
        keys = pair.T[HD:, :]
        lane = lanes_of((N, LANES))
        values = PROJ[block_rows(zz), LANES:].astype(jnp.float32)
        values = jnp.where(lane < HD, values, jnp.where(lane == HD, 1.0, 0.0)).astype(jnp.bfloat16)
        state = dot((keys * weights).astype(jnp.bfloat16), values)
        lane = lanes_of(state.shape)
        state = jnp.where(lane == HD + 1, passed, jnp.where(lane == HD + 2, level, state))
        ST[zz * Y + y] = state
        keys = keys.astype(jnp.bfloat16)
        summed_col = jnp.broadcast_to(summed, (LANES, N)).T
        source = log_in - summed
        lane = lanes_of(wide)
        for i in range(parts):
            width = (i + 1) * WINDOW
            span = (WINDOW, width)
            causal = lax.broadcasted_iota(jnp.int32, span, 0) + i * WINDOW >= lanes_of(span)
            since = summed_col[i * WINDOW : (i + 1) * WINDOW, :]
            log_weight = jnp.where(causal, since[:, :1] + source[:, :width], MASKED)
            peak = jnp.max(log_weight, axis=-1, keepdims=True)
            affinity = dot(query[i * WINDOW : (i + 1) * WINDOW], keys[:, :width]) * jnp.exp(
                log_weight - peak
            )
            total = jnp.sum(affinity, axis=-1, keepdims=True)
            found = dot(affinity.astype(jnp.bfloat16), values[:width])
            NUM[sub_rows(zz, i), :] = jnp.where(
                lane < HD, found,
                jnp.where(lane == HD, total, jnp.where(lane == HD + 1, peak, since)),
            )

    def local_work(zz):
        PROJ[block_rows(zz), :] = ACC[block_rows(zz), :CM].astype(jnp.bfloat16)

        @pl.when(holds)
        def _():
            PROJA[block_rows(zz), :] = ACCA[block_rows(zz), :].astype(jnp.bfloat16)

        with jax.named_scope('remember'):
            remember(zz)

        @pl.when(holds)
        def _():
            h_side(zz, (y + 1) // Y).start()
            with jax.named_scope('attend'):
                for i in range(1, parts):
                    before = PROJA[sub_rows(zz, i - 1), CA - LANES :]
                    for pair in range(CA // LANES - 1):
                        attend(zz, i, before, pair)

        for k in range(1, Y):
            s_side(zz, k, y).start()

    def near(d, act):
        pl.when((z == d) & can_up)(lambda: weights_out(0, 1, act))
        pl.when((z == Z - 1 - d) & can_down)(lambda: weights_out(1, 1, act))

    own_tokens(begin)
    with jax.named_scope('pack'):
        pack()
    for k in range(1, Z):
        f_across(k, z).start()
    weights_aside(z, begin)
    output_aside(begin)
    near(0, begin)
    ACC[...] = jnp.zeros_like(ACC)
    ACCA[...] = jnp.zeros_like(ACCA)

    def turn(i, nothing):
        cols = pl.ds(pl.multiple_of(i * LANES, LANES), LANES)
        count = gates.shape[0]
        tall = jnp.concatenate(
            [gates[:, cols].astype(jnp.float32), jnp.zeros((LANES - count, LANES), jnp.float32)],
            axis=0,
        )
        GW[cols, :] = tall.T.astype(jnp.bfloat16)
        return nothing

    lax.fori_loop(0, D // LANES, turn, 0)

    def both_sides(d, act):
        def one(side, nothing):
            zz = z + d * (2 * side - 1)
            pl.when((zz >= 0) & (zz < Z) & (d + 1 - side > 0))(lambda: act(zz))
            return nothing

        lax.fori_loop(0, 2, one, 0)

    def arrived(zz):
        for k in range(XH):
            for c in range(TC):
                t_twin(zz, k, c, (twin + TP - 2 * k) % TP).wait_recv()

    def weights_here(zz):
        for j in range(1, Y):
            for c in range(MC):
                m_side(zz, j, c, back_y(j)).wait_recv()

            @pl.when(holds)
            def _():
                for c in range(WC):
                    a_side(zz, j, c, back_y(j)).wait_recv()

    def early(zz):
        arrived(zz)
        project(z, zz)

    def stage(d, nothing):
        with jax.named_scope('t_on'):
            pl.when(d < Z - 1)(lambda: tokens_on(d, begin))
            pl.when(d == Z - 1)(lambda: tokens_on(d, begin, range(TC)))
        near(d, begin)
        inside = can_up & can_down

        @pl.when(d == Z - 1)
        def _():
            weights_far(begin)
            own_output(begin)
            with jax.named_scope('t_on_rest'):
                tokens_on(d, begin, range(TC, TC))

        @pl.when((d == 2) & inside)
        def _():
            with jax.named_scope('w_on_mid'):
                weights_on(1, begin)

        @pl.when(d == Z - 1)
        def _():
            with jax.named_scope('early'):
                weights_here(z)
                for near_d in range(Z - 2):
                    both_sides(near_d, early)

        with jax.named_scope('t_aside'):
            both_sides(d - 1, lambda zz: tokens_aside(zz, begin))
        return nothing

    lax.fori_loop(1, Z, stage, 0)
    with jax.named_scope('w_on_3'):
        for d in range(Z - 1, 2, -1):
            weights_on(d, begin)
    with jax.named_scope('t_last'):
        both_sides(Z - 1, lambda zz: tokens_aside(zz, begin))
        for d in range(max(Z - 2, 0), Z):
            both_sides(d, arrived)

    def multiply(zz):
        with jax.named_scope('w_side'):
            weights_here(zz)
        with jax.named_scope('project'):
            project_all(zz)

    def late(zz):
        project(z, zz)

    for d in range(max(Z - 2, 0), Z):
        both_sides(d, late)

    @pl.when(jnp.logical_not(can_up & can_down))
    def _():
        with jax.named_scope('w_on_1'):
            weights_on(1, begin)

    for d in range(Z - 1, 2, -1):
        both_sides(d, multiply)
    if Z > 2:
        with jax.named_scope('w_on_2'):
            weights_on(2, begin)
    for d in range(1, min(Z, 3)):
        both_sides(d, multiply)
    for k in range(1, Z):
        f_across(k, back_z(k)).wait_recv()

    with jax.named_scope('o_line_1'):
        output_on(1, begin, aside=False)

    def local(zz, nothing):
        local_work(zz)
        for i in range(2):
            pl.when(zz == Z - 3 + 2 * i)(lambda: output_pieces(i, 1 + i, begin))
        return nothing

    lax.fori_loop(0, Z, local, 0)

    output_pieces(2, 2 * OC, begin)

    with jax.named_scope('halo_state'):
        for zz in range(Z):
            pl.when(holds)(lambda: h_side(zz, 1 - jnp.minimum(y, 1)).wait_recv())
            for k in range(1, Y):
                s_side(zz, k, back_y(k)).wait_recv()

    def enter():
        carried = jnp.zeros((HD, LANES), jnp.float32)
        stabilizer = jnp.full((1, 1), MASKED, jnp.float32)
        lane = lanes_of((HD, LANES))
        for i in range(S):
            @pl.when(y == i % Y)
            def _(carried=carried, stabilizer=stabilizer):
                EB[i // Y] = jnp.where(lane == HD + 1, stabilizer, carried)

            state = ST[i]
            passed, level = state[0:1, HD + 1 : HD + 2], state[0:1, HD + 2 : HD + 3]
            newer = jnp.maximum(stabilizer + passed, level)
            carried = carried * jnp.exp(stabilizer + passed - newer) + state * jnp.exp(level - newer)
            stabilizer = newer

    enter()

    def finish(zz):
        @pl.when(holds)
        def _():
            for pair in range(CA // LANES - 1):
                attend(zz, 0, HALO[zz], pair)

        entering = EB[zz]
        stabilizer = entering[0:1, HD + 1 : HD + 2]
        local = NUM[block_rows(zz), :]
        peak, since = local[:, HD + 1 : HD + 2], local[:, HD + 2 : HD + 3]
        pair = PROJ[block_rows(zz), :LANES].astype(jnp.float32)
        query = (pair[:, :HD] * HD ** (-0.5)).astype(jnp.bfloat16)
        carried = dot(query, entering.astype(jnp.bfloat16))
        older = since + stabilizer
        row_level = jnp.maximum(older, peak)
        found = jnp.exp(older - row_level) * carried + jnp.exp(peak - row_level) * local
        bound = jnp.maximum(jnp.abs(found[:, HD : HD + 1]), jnp.exp(-row_level))
        gate = pltpu.roll(
            PROJ[block_rows(zz), LANES:].astype(jnp.float32), HD, 1
        )
        recall = found / bound * jax.nn.sigmoid(gate)
        half = N // 2
        lane = lanes_of((half, LANES))
        paired = jnp.where(lane < HD, recall[:half], pltpu.roll(recall[half:], HD, 1))
        JSM[zz] = paired.astype(jnp.bfloat16)

    def hand_over(k, act):
        act(j_across(k, z))

        @pl.when(holds)
        def _():
            act(ja_across(k, z - offset))
            act(l_across(k, z - offset))

    for k in range(1, Z):
        with jax.named_scope('finish'):
            finish(up_z(k))
        hand_over(k, begin)
    with jax.named_scope('finish'):
        finish(z)
    JM[tp, z] = JSM[z]

    @pl.when(holds)
    def _():
        JA[tp, z - offset] = JSA[z]
        LT[z - offset] = LS[z]

    def share(k, act):
        zz = back_z(k)
        if k and act is begin:
            j_across(k, zz).wait_recv()
        for j in range(1, XH):
            act(j_side(zz, j, tp))
        act(j_twin(zz, 0, tp))

        @pl.when(is_holder(zz))
        def _():
            if k and act is begin:
                ja_across(k, zz - offset).wait_recv()
            for j in range(1, XH):
                act(ja_side(zz - offset, j, tp))
            act(ja_twin(zz - offset, 0, tp))

    def share_aside(act):
        for zz in range(Z):
            for j in range(1, XH):
                if act is begin:
                    j_side(zz, j, from_tp(j)).wait_recv()
                act(j_twin(zz, j, from_tp(j)))
        for a in range(HOLD):
            for j in range(1, XH):
                if act is begin:
                    ja_side(a, j, from_tp(j)).wait_recv()
                act(ja_twin(a, j, from_tp(j)))

    share(0, begin)

    def settle():
        own_tokens(drain)
        weights_far(drain)
        weights_aside(z, drain)
        for k in range(1, Z):
            f_across(k, z).wait_send()
        for d in range(Z):
            near(d, drain)

        def one(i, nothing):
            weights_on(i, drain)
            tokens_on(i, drain)
            return nothing

        lax.fori_loop(1, Z, one, 0)

        def two(zz, nothing):
            tokens_aside(zz, drain)
            pl.when(holds)(lambda: h_side(zz, (y + 1) // Y).wait_send())
            for k in range(1, Y):
                s_side(zz, k, y).wait_send()
            return nothing

        lax.fori_loop(0, Z, two, 0)
        output_aside(drain)
        own_output(drain)

    with jax.named_scope('settle'):
        settle()
    for d in range(2, Z):
        with jax.named_scope('o_on_2'):
            output_on(d, begin)
        if d == 2:
            with jax.named_scope('share'):
                for k in range(1, Z):
                    share(k, begin)
            with jax.named_scope('share_aside'):
                share_aside(begin)
    with jax.named_scope('share_wait'):
        for k in range(1, Z):
            origin = back_z(k)
            pl.when(is_holder(origin))(lambda: l_across(k, origin - offset).wait_recv())
        for k in range(XH):
            for zz in range(Z):
                j_twin(zz, k, (twin + TP - 2 * k) % TP).wait_recv()
            for a in range(HOLD):
                ja_twin(a, k, (twin + TP - 2 * k) % TP).wait_recv()

    mem_base = TP * sinks.shape[0] * HD
    per_tp = sinks.shape[0] * HD
    half = N // 2
    pairs = CA // LANES - 1
    for t in range(TP):
        for a in range(HOLD):
            for pair in range(pairs):
                at = t * per_tp + (a * pairs + pair) * LANES
                X[:, at : at + LANES] = JA[t, a, pair * N : (pair + 1) * N, :]
        for zz in range(Z):
            at = mem_base + (t * Z + zz) * HD
            X[:half, at : at + HD] = JM[t, zz, :, :HD]
            X[half:, at : at + HD] = JM[t, zz, :, HD:]
    for a in range(HOLD):
        totals[2 * pairs * a : 2 * pairs * (a + 1), :] = LT[a, : 2 * pairs, :]

    tile = min(256, M)
    deep = Y * KO

    def outputs(zz):
        for k in range(1, Y):
            for c in range(OC):
                o_side(zz, k, c, back_y(k), False).wait_recv()
        part = pl.ds(pl.multiple_of(zz * deep, deep), deep)

        def columns(i, nothing):
            cols = pl.ds(pl.multiple_of(i * tile, tile), tile)
            MIX[:, cols] += dot(X[:, part], O[part, cols])
            return nothing

        lax.fori_loop(0, M // tile, columns, 0)

    MIX[...] = jnp.zeros_like(MIX)
    with jax.named_scope('settle_j'):
        output_on(1, drain)
        for k in range(1, Z):
            hand_over(k, drain)
        for k in range(Z):
            share(k, drain)
        share_aside(drain)
    keep[7].wait()

    def stage_three(d, nothing):
        with jax.named_scope('outputs'):
            both_sides(d, outputs)
        return nothing

    lax.fori_loop(0, Z, stage_three, 0)
    with jax.named_scope('cast'):
        mixed[...] = MIX[...].astype(jnp.bfloat16)

    with jax.named_scope('drain'):
        for d in range(2, Z):
            output_on(d, drain)


def mix(tokens, gain, shifts, gates, w_out, weights, sinks, bias):
    S, TP = lax.axis_size("sp"), lax.axis_size("tp")
    Z = shifts.shape[0]
    Y, XH = S // Z, TP // 2
    R, D = tokens.shape
    N = R * TP
    KD = weights[0].shape[0]
    HOLD = weights[1].shape[1] // HD
    CA = weights[0].shape[1] // HOLD + 2 * HD
    CM = sum(part.shape[1] for part in weights[3:]) // Z
    MC = 2
    TC = OC = 3
    WC = 4
    M = w_out.shape[1]
    bf, f32 = jnp.bfloat16, jnp.float32
    dma = pltpu.SemaphoreType.DMA
    vmem = pl.BlockSpec(memory_space=pltpu.VMEM)
    smem = pl.BlockSpec(memory_space=pltpu.SMEM)
    hbm = pl.BlockSpec(memory_space=pl.ANY)
    return pl.pallas_call(
        functools.partial(mixer_kernel, (Z, Y, TP, TC, WC, OC)),
        out_shape=[
            jax.ShapeDtypeStruct((N, M), bf),
            jax.ShapeDtypeStruct((sinks.shape[0], N), f32),
        ],
        in_specs=[vmem] * 4 + [hbm] * 8 + [smem] * 2,
        out_specs=[vmem] * 2,
        scratch_shapes=[pltpu.VMEM(part.shape, bf) for part in weights]
        + [
            pltpu.VMEM((Z, KD, CM), bf),
            pltpu.VMEM((HOLD, KD, CA), bf),
            pltpu.VMEM((Z * N, D), bf),
            pltpu.VMEM((D, CM), bf),
            pltpu.VMEM((D, CA), bf),
            pltpu.VMEM((D, LANES), bf),
            pltpu.VMEM((S * w_out.shape[0], M), bf),
            pltpu.VMEM((Z * N, CM + LANES), f32),
            pltpu.VMEM((Z * N, CA), f32),
            pltpu.VMEM((LANES, N), f32),
            pltpu.VMEM((Z * N, CM), bf),
            pltpu.VMEM((Z * N, CA), bf),
            pltpu.VMEM((Z * N, LANES), f32),
            pltpu.VMEM((S, HD, LANES), f32),
            pltpu.VMEM((Z, HD, LANES), f32),
            pltpu.VMEM((Z + 1, WINDOW, LANES), bf),
            pltpu.VMEM((Z, 8, N), f32),
            pltpu.VMEM((Z, 8, N), f32),
            pltpu.VMEM((Z, N // 2, LANES), bf),
            pltpu.VMEM((Z, N * (CA // LANES - 1), LANES), bf),
            pltpu.VMEM((TP, Z, N // 2, LANES), bf),
            pltpu.VMEM((TP, HOLD, N * (CA // LANES - 1), LANES), bf),
            pltpu.VMEM((Z, 8, N), f32),
            pltpu.VMEM((HOLD, 8, N), f32),
            pltpu.VMEM((N, S * w_out.shape[0]), bf),
            pltpu.VMEM((N, M), f32),
            dma((8,)),
            dma((Z,)), dma((Z, MC)), dma((Z,)), dma((Z, WC)),
            dma((Y - 1, Z)), dma((Y - 1, Z, MC)), dma((Y - 1, Z)), dma((Y - 1, Z, WC)),
            dma((Z,)), dma((Z,)),
            dma((2, Z)), dma((Z, TC)), dma((XH - 1, Z)), dma((XH - 1, Z, TC)),
            dma((XH, Z)), dma((XH, Z, TC)),
            dma((2, Z)), dma((Z, OC)), dma((Y - 1, Z)), dma((Y - 1, Z, OC)),
            dma((Z,)), dma((Z,)), dma((Y - 1, Z)), dma((Y - 1, Z)),
            dma((Z,)), dma((Z,)), dma((Z,)), dma((Z,)), dma((Z,)), dma((Z,)),
            dma((XH - 1, Z)), dma((XH - 1, Z)), dma((XH, Z)), dma((XH, Z)),
            dma((XH - 1, HOLD)), dma((XH - 1, HOLD)), dma((XH, HOLD)), dma((XH, HOLD)),
        ],
        compiler_params=pltpu.CompilerParams(
            collective_id=0, has_side_effects=True, vmem_limit_bytes=60 * 2**20
        ),
    )(tokens, gain, shifts, gates, w_out, *weights, sinks, bias)


def shards(
    tokens,
    norm_gain,
    w_query,
    w_key,
    w_value,
    w_mem_query,
    w_mem_key,
    w_mem_value,
    w_mem_gate,
    w_gates,
    sinks,
    forget_bias,
    forget_shift,
    w_out,
):
    weights = (w_query, w_key, w_value, w_mem_query, w_mem_key, w_mem_value, w_mem_gate)
    mixed, totals = mix(
        tokens,
        norm_gain[None, :],
        forget_shift.T,
        w_gates.transpose(1, 2, 0).reshape(-1, w_gates.shape[0]),
        w_out,
        weights,
        sinks,
        forget_bias,
    )
    return mixed, totals.T


def solution(mesh):
    placed = (
        P(("sp", "tp"), None),
        P(),
        P("sp", "tp"),
        P("sp", "tp"),
        P("sp", "tp"),
        P("sp", "tp"),
        P("sp", "tp"),
        P("sp", "tp"),
        P("sp", "tp"),
        P(),
        P("tp"),
        P("tp"),
        P("sp", "tp"),
        P("sp", "tp"),
    )
    return jax.shard_map(
        shards,
        mesh=mesh,
        in_specs=placed,
        out_specs=(P("sp", "tp"), P("sp", "tp")),
        check_vma=False,
    )
```

```python
import functools
import math

import jax
import jax.numpy as jnp
from jax import lax
from jax.experimental import pallas as pl
from jax.experimental.pallas import tpu as pltpu
from jax.sharding import PartitionSpec as P

HD = 64
WINDOW = 128
LANES = 128
EPSILON = 1e-06
MASKED = -1e30
MESH = pl.DeviceIdType.MESH


def begin(copy):
    copy.start()


def drain(copy):
    copy.wait_send()


def each(count, act):
    return range(count) if act is begin else (None,)


def dot(left, right, **more):
    return jnp.dot(left, right, preferred_element_type=jnp.float32, **more)


def lanes_of(shape):
    return lax.broadcasted_iota(jnp.int32, shape, len(shape) - 1)


def mixer_kernel(
    sizes,
    tokens, gain, shifts, gates, w_out, w_query, w_key, w_value, w_mem_query, w_mem_key,
    w_mem_value, w_mem_gate, sinks, bias,
    mixed, totals,
    in_query, in_key, in_value, in_mem_query, in_mem_key, in_mem_value, in_mem_gate,
    PM, PA, T, WM, WA, GW, O, ACC, ACCA, FLAT, PROJ, PROJA, NUM, ST, EB, HALO, SH, FS,
    JSM, JSA, JM, JA, LS, LT, X, MIX,
    own_sems, w_send, w_recv, wa_send, wa_recv, wy_send, wy_recv, wb_send, wb_recv,
    f_send, f_recv, tz_send, tz_recv, tx_send, tx_recv, tt_send, tt_recv,
    oz_send, oz_recv, oy_send, oy_recv, h_send, h_recv, s_send, s_recv,
    jz_send, jz_recv, ja_send, ja_recv, l_send, l_recv,
    jx_send, jx_recv, jt_send, jt_recv, jxa_send, jxa_recv, jta_send, jta_recv,
):
    Z, Y, TP, TC, WC, OC = sizes
    XH = TP // 2
    R, D = tokens.shape
    N = R * TP
    HOLD, KD, CA = PA.shape
    CM = PM.shape[2]
    offset = (Z - HOLD) // 2
    KO, M = w_out.shape
    MC = WC // 2
    RC, RW, RM, RO = R // TC, KD // WC, KD // MC, KO // OC
    S = Z * Y
    sp, tp = lax.axis_index("sp"), lax.axis_index("tp")
    z, y = sp // Y, sp % Y
    twin = tp + 1 - 2 * (tp % 2)

    def is_holder(zz):
        return (zz >= offset) & (zz < offset + HOLD)

    holds = is_holder(z)
    can_up, can_down = z < Z - 1, z > 0

    def remote(src, dst, send, recv, to_sp, to_tp):
        return pltpu.make_async_remote_copy(
            src_ref=src, dst_ref=dst, send_sem=send, recv_sem=recv,
            device_id={"sp": to_sp, "tp": to_tp}, device_id_type=MESH,
        )

    def span(base, c, count, size):
        if c is None:
            return pl.ds(pl.multiple_of(base, size), count * size)
        return pl.ds(pl.multiple_of(base + c * size, size), size)

    def slot(c):
        return 0 if c is None else c

    def side_tp(k):
        return (tp + 2 * k) % TP

    def from_tp(k):
        return (tp + TP - 2 * k) % TP

    def up_z(k):
        return (z + k) % Z

    def back_z(k):
        return (z + Z - k) % Z

    def up_y(k):
        return (y + k) % Y

    def back_y(k):
        return (y + Y - k) % Y

    def m_rows(zz, yy, c):
        return WM.at[span((zz * Y + yy) * KD, c, MC, RM), :]

    def a_rows(zz, yy, c):
        return WA.at[span((zz * Y + yy) * KD, c, WC, RW), :]

    def m_across(way, d, c, source, piece):
        to = z + d * (1 - 2 * way)
        return remote(
            PM.at[piece, span(0, c, MC, RM), :], m_rows(source, y, c),
            w_send.at[to], w_recv.at[source, slot(c)], to * Y + y, tp,
        )

    def a_across(way, d, c, source, piece):
        to = z + d * (1 - 2 * way)
        return remote(
            PA.at[piece, span(0, c, WC, RW), :], a_rows(source, y, c),
            wa_send.at[to], wa_recv.at[source, slot(c)], to * Y + y, tp,
        )

    def m_side(zz, j, c, source):
        place = m_rows(zz, source, c)
        return remote(
            place, place, wy_send.at[j - 1, zz], wy_recv.at[j - 1, zz, slot(c)], z * Y + up_y(j), tp
        )

    def a_side(zz, j, c, source):
        place = a_rows(zz, source, c)
        return remote(
            place, place, wb_send.at[j - 1, zz], wb_recv.at[j - 1, zz, slot(c)], z * Y + up_y(j), tp
        )

    def f_across(k, source):
        return remote(
            SH.at[up_z(k)], FS.at[source], f_send.at[k], f_recv.at[k], up_z(k) * Y + y, tp
        )

    def t_rows(zz, tt, c):
        return T.at[span((zz * TP + tt) * R, c, TC, RC), :]

    def t_line(zz, way, c):
        place = t_rows(zz, tp, c)
        to = (z + 1 - 2 * way) * Y + y
        return remote(place, place, tz_send.at[way, zz], tz_recv.at[zz, slot(c)], to, tp)

    def t_side(zz, k, c, source):
        place = t_rows(zz, source, c)
        return remote(place, place, tx_send.at[k - 1, zz], tx_recv.at[k - 1, zz, slot(c)], sp, side_tp(k))

    def t_twin(zz, k, c, source):
        place = t_rows(zz, source, c)
        return remote(place, place, tt_send.at[k, zz], tt_recv.at[k, zz, slot(c)], sp, twin)

    def o_rows(zz, yy, c):
        return O.at[span((zz * Y + yy) * KO, c, OC, RO), :]

    def o_line(zz, way, c, own):
        place = o_rows(zz, y, c)
        src = w_out.at[span(0, c, OC, RO), :] if own else place
        to = (z + 1 - 2 * way) * Y + y
        return remote(src, place, oz_send.at[way, zz], oz_recv.at[zz, slot(c)], to, tp)

    def o_side(zz, k, c, source, own):
        place = o_rows(zz, source, c)
        src = w_out.at[span(0, c, OC, RO), :] if own else place
        return remote(src, place, oy_send.at[k - 1, zz], oy_recv.at[k - 1, zz, slot(c)], z * Y + up_y(k), tp)

    def h_side(zz, shift):
        rows = pl.ds(pl.multiple_of(zz * N + N - WINDOW, WINDOW), WINDOW)
        return remote(
            PROJA.at[rows, pl.ds(CA - LANES, LANES)], HALO.at[zz + shift],
            h_send.at[zz], h_recv.at[zz], z * Y + up_y(1), tp,
        )

    def s_side(zz, k, source):
        place = ST.at[zz * Y + source]
        return remote(place, place, s_send.at[k - 1, zz], s_recv.at[k - 1, zz], z * Y + up_y(k), tp)

    def j_across(k, source):
        return remote(
            JSM.at[up_z(k)], JM.at[tp, source], jz_send.at[k], jz_recv.at[k], up_z(k) * Y + y, tp
        )

    def ja_across(k, holder):
        return remote(
            JSA.at[up_z(k)], JA.at[tp, holder], ja_send.at[k], ja_recv.at[k], up_z(k) * Y + y, tp
        )

    def l_across(k, holder):
        return remote(
            LS.at[up_z(k)], LT.at[holder], l_send.at[k], l_recv.at[k], up_z(k) * Y + y, tp
        )

    def j_side(zz, k, source):
        place = JM.at[source, zz]
        return remote(place, place, jx_send.at[k - 1, zz], jx_recv.at[k - 1, zz], sp, side_tp(k))

    def j_twin(zz, k, source):
        place = JM.at[source, zz]
        return remote(place, place, jt_send.at[k, zz], jt_recv.at[k, zz], sp, twin)

    def ja_side(a, k, source):
        place = JA.at[source, a]
        return remote(place, place, jxa_send.at[k - 1, a], jxa_recv.at[k - 1, a], sp, side_tp(k))

    def ja_twin(a, k, source):
        place = JA.at[source, a]
        return remote(place, place, jta_send.at[k, a], jta_recv.at[k, a], sp, twin)

    ins = (
        (w_query, in_query), (w_key, in_key), (w_value, in_value), (w_mem_query, in_mem_query),
        (w_mem_key, in_mem_key), (w_mem_value, in_mem_value), (w_mem_gate, in_mem_gate),
        (w_out, O.at[pl.ds(pl.multiple_of(sp * KO, KO), KO), :]),
    )
    keep = [pltpu.make_async_copy(a, b, own_sems.at[i]) for i, (a, b) in enumerate(ins)]

    barrier = pltpu.get_barrier_semaphore()
    greeted = [(up_z(k) * Y + y, tp) for k in range(1, Z)]
    greeted += [(z * Y + up_y(k), tp) for k in range(1, Y)]
    greeted += [(sp, side_tp(k)) for k in range(1, XH)] + [(sp, twin)]
    for to_sp, to_tp in greeted:
        pl.semaphore_signal(
            barrier, inc=1, device_id={"sp": to_sp, "tp": to_tp}, device_id_type=MESH
        )
    for copy in keep:
        copy.start()

    step = 16
    for i in range(R // step):
        values = tokens[pl.ds(i * step, step), :].astype(jnp.float32)
        rescale = lax.rsqrt(jnp.mean(values * values, axis=-1, keepdims=True) + EPSILON)
        start = pl.multiple_of((z * TP + tp) * R + i * step, step)
        T[pl.ds(start, step), :] = (values * rescale * gain[...]).astype(jnp.bfloat16)
    for i in range(Z):
        SH[i, 0:1, :] = shifts[i : i + 1, :]
    FS[z] = SH[z]

    @pl.when(y == 0)
    def _():
        HALO[0] = jnp.zeros(HALO.shape[1:], HALO.dtype)

    with jax.named_scope('barrier_wait'):
        pl.semaphore_wait(barrier, len(greeted))

    def pack():
        for copy in keep[:7]:
            copy.wait()
        high = min(KD, WINDOW)
        lane = lanes_of((high, LANES))
        qa = CA - LANES

        def halves(rows, left, i, right, j):
            a = left[rows, pl.ds(i // 2 * LANES, LANES)].astype(jnp.float32)
            b = right[rows, pl.ds(j // 2 * LANES, LANES)].astype(jnp.float32)
            a = pltpu.roll(a, HD, 1) if i % 2 else a
            b = b if j % 2 else pltpu.roll(b, HD, 1)
            return jnp.where(lane < HD, a, b).astype(jnp.bfloat16)

        def some(r, nothing):
            rows = pl.ds(pl.multiple_of(r * high, high), high)
            for i in range(Z):
                PM[i, rows, :LANES] = halves(rows, in_mem_query, i, in_mem_key, i)
                PM[i, rows, LANES:] = halves(rows, in_mem_value, i, in_mem_gate, i)
            for i in range(HOLD):
                PA[i, rows, :qa] = in_query[rows, i * qa : (i + 1) * qa]
                PA[i, rows, qa:] = halves(rows, in_key, i, in_value, i)
            return nothing

        lax.fori_loop(0, KD // high, some, 0)
        rows = pl.ds(pl.multiple_of(sp * KD, KD), KD)
        WM[rows, :] = PM[z]

        @pl.when(holds)
        def _():
            WA[rows, :] = PA[z - offset]

    def ways(d):
        return ((0, z + d < Z, z - d >= 0), (1, z - d >= 0, z + d < Z))

    def weights_out(way, d, act):
        to = z + d * (1 - 2 * way)

        @pl.when(is_holder(to))
        def _():
            for c in each(WC, act):
                act(a_across(way, d, c, z, to - offset))

        for c in each(MC, act):
            act(m_across(way, d, c, z, to))

    def weights_far(act):
        for d in range(Z - 1, 1, -1):
            for way, there, _ in ways(d):
                pl.when(there)(lambda: weights_out(way, d, act))

    def weights_aside(zz, act):
        for j in range(1, Y):
            for c in each(MC, act):
                act(m_side(zz, j, c, y))

            @pl.when(holds)
            def _():
                for c in each(WC, act):
                    act(a_side(zz, j, c, y))

    def weights_on(d, act):
        for way, _, there in ways(d):
            origin = z - d * (1 - 2 * way)

            def landed_a(way=way, origin=origin):
                for c in each(WC, act):
                    if act is begin:
                        a_across(way, d, c, origin, 0).wait_recv()
                    for j in range(1, Y):
                        act(a_side(origin, j, c, y))

            def landed_m(way=way, origin=origin):
                for c in each(MC, act):
                    if act is begin:
                        m_across(way, d, c, origin, 0).wait_recv()
                    for j in range(1, Y):
                        act(m_side(origin, j, c, y))

            pl.when(there & holds)(landed_a)
            pl.when(there)(landed_m)

    def own_tokens(act):
        for c in each(TC, act):
            pl.when(can_up)(lambda: act(t_line(z, 0, c)))
            pl.when(can_down)(lambda: act(t_line(z, 1, c)))
            for k in range(1, XH):
                act(t_side(z, k, c, tp))
            act(t_twin(z, 0, c, tp))

    def tokens_on(d, act, some=None):
        for way, origin, there, further in (
            (0, z - d, z - d >= 0, can_up), (1, z + d, z + d < Z, can_down),
        ):
            def landed(way=way, origin=origin, further=further):
                for c in each(TC, act) if some is None else some:
                    if act is begin:
                        t_line(origin, way, c).wait_recv()
                    pl.when(further)(lambda: act(t_line(origin, way, c)))
                    for k in range(1, XH):
                        act(t_side(origin, k, c, tp))
                    act(t_twin(origin, 0, c, tp))

            pl.when(there)(landed)

    def tokens_aside(zz, act):
        for k in range(1, XH):
            for c in each(TC, act):
                if act is begin:
                    t_side(zz, k, c, from_tp(k)).wait_recv()
                act(t_twin(zz, k, c, from_tp(k)))

    def output_aside(act):
        for c in each(OC, act):
            for k in range(1, Y):
                act(o_side(z, k, c, y, True))

    def own_output(act):
        for c in each(OC, act):
            pl.when(can_up)(lambda: act(o_line(z, 0, c, True)))
            pl.when(can_down)(lambda: act(o_line(z, 1, c, True)))

    def output_on(d, act, line=True, aside=True):
        for way, origin, there, further in (
            (0, z - d, z - d >= 0, can_up), (1, z + d, z + d < Z, can_down),
        ):
            def landed(way=way, origin=origin, further=further):
                for c in each(OC, act):
                    if act is begin and line:
                        o_line(origin, way, c, False).wait_recv()
                    if line:
                        pl.when(further)(lambda: act(o_line(origin, way, c, False)))
                    if aside:
                        for k in range(1, Y):
                            act(o_side(origin, k, c, y, False))

            pl.when(there)(landed)

    def output_pieces(first, last, act):
        for c, way in [(c, way) for c in range(OC) for way in range(2)][first:last]:
            origin = z - 1 + 2 * way

            @pl.when((origin >= 0) & (origin < Z))
            def _():
                for k in range(1, Y):
                    act(o_side(origin, k, c, y, False))

    def block_rows(zz):
        return pl.ds(pl.multiple_of(zz * N, N), N)

    depth = Y * KD

    def project(zk, b):
        cols = pl.ds(pl.multiple_of(zk * depth, depth), depth)

        rows = block_rows(b)
        block = T[rows, cols]
        ACC[rows, :CM] += dot(block, WM[cols, :])
        ACC[rows, CM:] += dot(block, GW[cols, :])

        @pl.when(holds)
        def _():
            ACCA[rows, :] += dot(block, WA[cols, :])

    def project_all(zk):
        def part(b, nothing):
            project(zk, b)
            return nothing

        lax.fori_loop(0, Z, part, 0)

    parts = N // WINDOW
    wide = (WINDOW, LANES)

    def sub_rows(zz, i):
        return pl.ds(pl.multiple_of(zz * N + i * WINDOW, WINDOW), WINDOW)

    def attend(zz, i, before, pair):
        lane = lanes_of(wide)
        heads = PROJA[sub_rows(zz, i), pair * LANES : (pair + 1) * LANES].astype(jnp.float32) * HD ** (-0.5)
        first = jnp.where(lane < HD, heads, 0.0)
        second = jnp.where(lane < HD, pltpu.roll(heads, HD, 1), 0.0)
        query = jnp.concatenate([first, second], axis=0).astype(jnp.bfloat16)
        rows = jnp.concatenate([before, PROJA[sub_rows(zz, i), CA - LANES :]], axis=0)
        scores = lax.dot_general(
            query, rows, (((1,), (1,)), ((), ())), preferred_element_type=jnp.float32
        )
        shape = (2 * WINDOW, 2 * WINDOW)
        at = lax.broadcasted_iota(jnp.int32, shape, 0)
        head = at >= WINDOW
        key_at = lax.broadcasted_iota(jnp.int32, shape, 1)
        distance = jnp.where(head, at - WINDOW, at) - key_at + WINDOW
        allowed = (distance >= 0) & (distance < WINDOW)
        if i == 0:
            lowest = WINDOW * (1 - jnp.minimum(zz * Y + y, 1))
            allowed = allowed & (key_at >= lowest)
        scores = jnp.where(allowed, scores, MASKED)
        tall = lax.broadcasted_iota(jnp.int32, (2 * WINDOW, 1), 0) >= WINDOW
        at_sink = (z - offset) * (CA - LANES) // HD + 2 * pair
        sink = jnp.where(tall, sinks[at_sink + 1], sinks[at_sink])
        ceiling = jnp.maximum(jnp.max(scores, axis=-1, keepdims=True), sink)
        weights = jnp.exp(scores - ceiling)
        total = jnp.exp(sink - ceiling) + jnp.sum(weights, axis=-1, keepdims=True)
        probs = (weights * (1.0 / total)).astype(jnp.bfloat16)
        out = dot(probs, rows)
        both = jnp.where(lane < HD, pltpu.roll(out[:WINDOW], HD, 1), out[WINDOW:])
        JSA[zz, pl.ds(pair * N + i * WINDOW, WINDOW), :] = both.astype(jnp.bfloat16)
        logs = jnp.broadcast_to(ceiling + jnp.log(total), (2 * WINDOW, LANES)).T
        LS[zz, 2 * pair : 2 * pair + 1, pl.ds(i * WINDOW, WINDOW)] = logs[0:1, :WINDOW]
        LS[zz, 2 * pair + 1 : 2 * pair + 2, pl.ds(i * WINDOW, WINDOW)] = logs[0:1, WINDOW:]

    def remember(zz):
        FLAT[...] = ACC[block_rows(zz), CM:].T
        gate_count = gates.shape[0] // 2
        head = tp * Z + z
        log_in = FLAT[pl.ds(head, 1), :] - 0.5 * math.log(N * S)
        pre = FLAT[pl.ds(gate_count + head, 1), :] + bias[z]
        log_sig = jnp.minimum(pre, 0.0) - jnp.log1p(jnp.exp(-jnp.abs(pre)))
        log_forget = log_sig + FS[zz][0:1, :]
        square = (N, N)
        before = lax.broadcasted_iota(jnp.int32, square, 0) <= lax.broadcasted_iota(
            jnp.int32, square, 1
        )
        summed = dot(
            jnp.broadcast_to(log_forget, (8, N)), before.astype(jnp.float32),
            precision=lax.Precision.HIGHEST,
        )[0:1, :]
        passed = summed[:, N - 1 :]
        decays = passed - summed + log_in
        level = jnp.max(decays, axis=1, keepdims=True)
        weights = jnp.exp(decays - level)
        pair = PROJ[block_rows(zz), :LANES].astype(jnp.float32)
        query = (pair[:, :HD] * HD ** (-0.5)).astype(jnp.bfloat16)
        keys = pair.T[HD:, :]
        lane = lanes_of((N, LANES))
        values = PROJ[block_rows(zz), LANES:].astype(jnp.float32)
        values = jnp.where(lane < HD, values, jnp.where(lane == HD, 1.0, 0.0)).astype(jnp.bfloat16)
        state = dot((keys * weights).astype(jnp.bfloat16), values)
        lane = lanes_of(state.shape)
        state = jnp.where(lane == HD + 1, passed, jnp.where(lane == HD + 2, level, state))
        ST[zz * Y + y] = state
        keys = keys.astype(jnp.bfloat16)
        summed_col = jnp.broadcast_to(summed, (LANES, N)).T
        source = log_in - summed
        lane = lanes_of(wide)
        for i in range(parts):
            width = (i + 1) * WINDOW
            span = (WINDOW, width)
            causal = lax.broadcasted_iota(jnp.int32, span, 0) + i * WINDOW >= lanes_of(span)
            since = summed_col[i * WINDOW : (i + 1) * WINDOW, :]
            log_weight = jnp.where(causal, since[:, :1] + source[:, :width], MASKED)
            peak = jnp.max(log_weight, axis=-1, keepdims=True)
            affinity = dot(query[i * WINDOW : (i + 1) * WINDOW], keys[:, :width]) * jnp.exp(
                log_weight - peak
            )
            total = jnp.sum(affinity, axis=-1, keepdims=True)
            found = dot(affinity.astype(jnp.bfloat16), values[:width])
            NUM[sub_rows(zz, i), :] = jnp.where(
                lane < HD, found,
                jnp.where(lane == HD, total, jnp.where(lane == HD + 1, peak, since)),
            )

    def local_work(zz):
        PROJ[block_rows(zz), :] = ACC[block_rows(zz), :CM].astype(jnp.bfloat16)

        @pl.when(holds)
        def _():
            PROJA[block_rows(zz), :] = ACCA[block_rows(zz), :].astype(jnp.bfloat16)

        with jax.named_scope('remember'):
            remember(zz)

        @pl.when(holds)
        def _():
            h_side(zz, (y + 1) // Y).start()
            with jax.named_scope('attend'):
                for i in range(1, parts):
                    before = PROJA[sub_rows(zz, i - 1), CA - LANES :]
                    for pair in range(CA // LANES - 1):
                        attend(zz, i, before, pair)

        for k in range(1, Y):
            s_side(zz, k, y).start()

    def near(d, act):
        pl.when((z == d) & can_up)(lambda: weights_out(0, 1, act))
        pl.when((z == Z - 1 - d) & can_down)(lambda: weights_out(1, 1, act))

    own_tokens(begin)
    with jax.named_scope('pack'):
        pack()
    for k in range(1, Z):
        f_across(k, z).start()
    weights_aside(z, begin)
    output_aside(begin)
    near(0, begin)
    ACC[...] = jnp.zeros_like(ACC)
    ACCA[...] = jnp.zeros_like(ACCA)

    def turn(i, nothing):
        cols = pl.ds(pl.multiple_of(i * LANES, LANES), LANES)
        count = gates.shape[0]
        tall = jnp.concatenate(
            [gates[:, cols].astype(jnp.float32), jnp.zeros((LANES - count, LANES), jnp.float32)],
            axis=0,
        )
        GW[cols, :] = tall.T.astype(jnp.bfloat16)
        return nothing

    lax.fori_loop(0, D // LANES, turn, 0)

    def both_sides(d, act):
        def one(side, nothing):
            zz = z + d * (2 * side - 1)
            pl.when((zz >= 0) & (zz < Z) & (d + 1 - side > 0))(lambda: act(zz))
            return nothing

        lax.fori_loop(0, 2, one, 0)

    def arrived(zz):
        for k in range(XH):
            for c in range(TC):
                t_twin(zz, k, c, (twin + TP - 2 * k) % TP).wait_recv()

    def weights_here(zz):
        for j in range(1, Y):
            for c in range(MC):
                m_side(zz, j, c, back_y(j)).wait_recv()

            @pl.when(holds)
            def _():
                for c in range(WC):
                    a_side(zz, j, c, back_y(j)).wait_recv()

    def early(zz):
        arrived(zz)
        project(z, zz)

    def stage(d, nothing):
        with jax.named_scope('t_on'):
            pl.when(d < Z - 1)(lambda: tokens_on(d, begin))
            pl.when(d == Z - 1)(lambda: tokens_on(d, begin, range(TC)))
        near(d, begin)
        inside = can_up & can_down

        @pl.when(d == Z - 1)
        def _():
            weights_far(begin)
            own_output(begin)
            with jax.named_scope('t_on_rest'):
                tokens_on(d, begin, range(TC, TC))

        @pl.when((d == 2) & inside)
        def _():
            with jax.named_scope('w_on_mid'):
                weights_on(1, begin)

        @pl.when(d == Z - 1)
        def _():
            with jax.named_scope('early'):
                weights_here(z)
                for near_d in range(Z - 2):
                    both_sides(near_d, early)

        with jax.named_scope('t_aside'):
            both_sides(d - 1, lambda zz: tokens_aside(zz, begin))
        return nothing

    lax.fori_loop(1, Z, stage, 0)
    with jax.named_scope('w_on_3'):
        for d in range(Z - 1, 2, -1):
            weights_on(d, begin)
    with jax.named_scope('t_last'):
        both_sides(Z - 1, lambda zz: tokens_aside(zz, begin))
        for d in range(max(Z - 2, 0), Z):
            both_sides(d, arrived)

    def multiply(zz):
        with jax.named_scope('w_side'):
            weights_here(zz)
        with jax.named_scope('project'):
            project_all(zz)

    def late(zz):
        project(z, zz)

    for d in range(max(Z - 2, 0), Z):
        both_sides(d, late)

    @pl.when(jnp.logical_not(can_up & can_down))
    def _():
        with jax.named_scope('w_on_1'):
            weights_on(1, begin)

    for d in range(Z - 1, 2, -1):
        both_sides(d, multiply)
    if Z > 2:
        with jax.named_scope('w_on_2'):
            weights_on(2, begin)
    for d in range(1, min(Z, 3)):
        both_sides(d, multiply)
    for k in range(1, Z):
        f_across(k, back_z(k)).wait_recv()

    with jax.named_scope('o_line_1'):
        output_on(1, begin, aside=False)
        output_pieces(0, 1, begin)

    def local(zz, nothing):
        local_work(zz)
        for i in range(1):
            pl.when(zz == Z - 1 + i)(lambda: output_pieces(1 + i, 1 + 1 + i, begin))
        return nothing

    lax.fori_loop(0, Z, local, 0)

    output_pieces(2, 2 * OC, begin)

    with jax.named_scope('halo_state'):
        for zz in range(Z):
            pl.when(holds)(lambda: h_side(zz, 1 - jnp.minimum(y, 1)).wait_recv())
            for k in range(1, Y):
                s_side(zz, k, back_y(k)).wait_recv()

    def enter():
        carried = jnp.zeros((HD, LANES), jnp.float32)
        stabilizer = jnp.full((1, 1), MASKED, jnp.float32)
        lane = lanes_of((HD, LANES))
        for i in range(S):
            @pl.when(y == i % Y)
            def _(carried=carried, stabilizer=stabilizer):
                EB[i // Y] = jnp.where(lane == HD + 1, stabilizer, carried)

            state = ST[i]
            passed, level = state[0:1, HD + 1 : HD + 2], state[0:1, HD + 2 : HD + 3]
            newer = jnp.maximum(stabilizer + passed, level)
            carried = carried * jnp.exp(stabilizer + passed - newer) + state * jnp.exp(level - newer)
            stabilizer = newer

    enter()

    def finish(zz):
        @pl.when(holds)
        def _():
            for pair in range(CA // LANES - 1):
                attend(zz, 0, HALO[zz], pair)

        entering = EB[zz]
        stabilizer = entering[0:1, HD + 1 : HD + 2]
        local = NUM[block_rows(zz), :]
        peak, since = local[:, HD + 1 : HD + 2], local[:, HD + 2 : HD + 3]
        pair = PROJ[block_rows(zz), :LANES].astype(jnp.float32)
        query = (pair[:, :HD] * HD ** (-0.5)).astype(jnp.bfloat16)
        carried = dot(query, entering.astype(jnp.bfloat16))
        older = since + stabilizer
        row_level = jnp.maximum(older, peak)
        found = jnp.exp(older - row_level) * carried + jnp.exp(peak - row_level) * local
        bound = jnp.maximum(jnp.abs(found[:, HD : HD + 1]), jnp.exp(-row_level))
        gate = pltpu.roll(
            PROJ[block_rows(zz), LANES:].astype(jnp.float32), HD, 1
        )
        recall = found / bound * jax.nn.sigmoid(gate)
        half = N // 2
        lane = lanes_of((half, LANES))
        paired = jnp.where(lane < HD, recall[:half], pltpu.roll(recall[half:], HD, 1))
        JSM[zz] = paired.astype(jnp.bfloat16)

    def hand_over(k, act):
        act(j_across(k, z))

        @pl.when(holds)
        def _():
            act(ja_across(k, z - offset))
            act(l_across(k, z - offset))

    for k in range(1, Z):
        with jax.named_scope('finish'):
            finish(up_z(k))
        hand_over(k, begin)
    with jax.named_scope('finish'):
        finish(z)
    JM[tp, z] = JSM[z]

    @pl.when(holds)
    def _():
        JA[tp, z - offset] = JSA[z]
        LT[z - offset] = LS[z]

    def share(k, act):
        zz = back_z(k)
        if k and act is begin:
            j_across(k, zz).wait_recv()
        for j in range(1, XH):
            act(j_side(zz, j, tp))
        act(j_twin(zz, 0, tp))

        @pl.when(is_holder(zz))
        def _():
            if k and act is begin:
                ja_across(k, zz - offset).wait_recv()
            for j in range(1, XH):
                act(ja_side(zz - offset, j, tp))
            act(ja_twin(zz - offset, 0, tp))

    def share_aside(act):
        for zz in range(Z):
            for j in range(1, XH):
                if act is begin:
                    j_side(zz, j, from_tp(j)).wait_recv()
                act(j_twin(zz, j, from_tp(j)))
        for a in range(HOLD):
            for j in range(1, XH):
                if act is begin:
                    ja_side(a, j, from_tp(j)).wait_recv()
                act(ja_twin(a, j, from_tp(j)))

    share(0, begin)

    def settle():
        own_tokens(drain)
        weights_far(drain)
        weights_aside(z, drain)
        for k in range(1, Z):
            f_across(k, z).wait_send()
        for d in range(Z):
            near(d, drain)

        def one(i, nothing):
            weights_on(i, drain)
            tokens_on(i, drain)
            return nothing

        lax.fori_loop(1, Z, one, 0)

        def two(zz, nothing):
            tokens_aside(zz, drain)
            pl.when(holds)(lambda: h_side(zz, (y + 1) // Y).wait_send())
            for k in range(1, Y):
                s_side(zz, k, y).wait_send()
            return nothing

        lax.fori_loop(0, Z, two, 0)
        output_aside(drain)
        own_output(drain)

    with jax.named_scope('settle'):
        settle()
    for d in range(2, Z):
        with jax.named_scope('o_on_2'):
            output_on(d, begin)
        if d == 2:
            with jax.named_scope('share'):
                for k in range(1, Z):
                    share(k, begin)
            with jax.named_scope('share_aside'):
                share_aside(begin)
    with jax.named_scope('share_wait'):
        for k in range(1, Z):
            origin = back_z(k)
            pl.when(is_holder(origin))(lambda: l_across(k, origin - offset).wait_recv())
        for k in range(XH):
            for zz in range(Z):
                j_twin(zz, k, (twin + TP - 2 * k) % TP).wait_recv()
            for a in range(HOLD):
                ja_twin(a, k, (twin + TP - 2 * k) % TP).wait_recv()

    mem_base = TP * sinks.shape[0] * HD
    per_tp = sinks.shape[0] * HD
    half = N // 2
    pairs = CA // LANES - 1
    for t in range(TP):
        for a in range(HOLD):
            for pair in range(pairs):
                at = t * per_tp + (a * pairs + pair) * LANES
                X[:, at : at + LANES] = JA[t, a, pair * N : (pair + 1) * N, :]
        for zz in range(Z):
            at = mem_base + (t * Z + zz) * HD
            X[:half, at : at + HD] = JM[t, zz, :, :HD]
            X[half:, at : at + HD] = JM[t, zz, :, HD:]
    for a in range(HOLD):
        totals[2 * pairs * a : 2 * pairs * (a + 1), :] = LT[a, : 2 * pairs, :]

    tile = min(256, M)
    deep = Y * KO

    def outputs(zz):
        for k in range(1, Y):
            for c in range(OC):
                o_side(zz, k, c, back_y(k), False).wait_recv()
        part = pl.ds(pl.multiple_of(zz * deep, deep), deep)

        def columns(i, nothing):
            cols = pl.ds(pl.multiple_of(i * tile, tile), tile)
            MIX[:, cols] += dot(X[:, part], O[part, cols])
            return nothing

        lax.fori_loop(0, M // tile, columns, 0)

    MIX[...] = jnp.zeros_like(MIX)
    with jax.named_scope('settle_j'):
        output_on(1, drain)
        for k in range(1, Z):
            hand_over(k, drain)
        for k in range(Z):
            share(k, drain)
        share_aside(drain)
    keep[7].wait()

    def stage_three(d, nothing):
        with jax.named_scope('outputs'):
            both_sides(d, outputs)
        return nothing

    lax.fori_loop(0, Z, stage_three, 0)
    with jax.named_scope('cast'):
        mixed[...] = MIX[...].astype(jnp.bfloat16)

    with jax.named_scope('drain'):
        for d in range(2, Z):
            output_on(d, drain)


def mix(tokens, gain, shifts, gates, w_out, weights, sinks, bias):
    S, TP = lax.axis_size("sp"), lax.axis_size("tp")
    Z = shifts.shape[0]
    Y, XH = S // Z, TP // 2
    R, D = tokens.shape
    N = R * TP
    KD = weights[0].shape[0]
    HOLD = weights[1].shape[1] // HD
    CA = weights[0].shape[1] // HOLD + 2 * HD
    CM = sum(part.shape[1] for part in weights[3:]) // Z
    MC = 2
    TC = OC = 3
    WC = 4
    M = w_out.shape[1]
    bf, f32 = jnp.bfloat16, jnp.float32
    dma = pltpu.SemaphoreType.DMA
    vmem = pl.BlockSpec(memory_space=pltpu.VMEM)
    smem = pl.BlockSpec(memory_space=pltpu.SMEM)
    hbm = pl.BlockSpec(memory_space=pl.ANY)
    return pl.pallas_call(
        functools.partial(mixer_kernel, (Z, Y, TP, TC, WC, OC)),
        out_shape=[
            jax.ShapeDtypeStruct((N, M), bf),
            jax.ShapeDtypeStruct((sinks.shape[0], N), f32),
        ],
        in_specs=[vmem] * 4 + [hbm] * 8 + [smem] * 2,
        out_specs=[vmem] * 2,
        scratch_shapes=[pltpu.VMEM(part.shape, bf) for part in weights]
        + [
            pltpu.VMEM((Z, KD, CM), bf),
            pltpu.VMEM((HOLD, KD, CA), bf),
            pltpu.VMEM((Z * N, D), bf),
            pltpu.VMEM((D, CM), bf),
            pltpu.VMEM((D, CA), bf),
            pltpu.VMEM((D, LANES), bf),
            pltpu.VMEM((S * w_out.shape[0], M), bf),
            pltpu.VMEM((Z * N, CM + LANES), f32),
            pltpu.VMEM((Z * N, CA), f32),
            pltpu.VMEM((LANES, N), f32),
            pltpu.VMEM((Z * N, CM), bf),
            pltpu.VMEM((Z * N, CA), bf),
            pltpu.VMEM((Z * N, LANES), f32),
            pltpu.VMEM((S, HD, LANES), f32),
            pltpu.VMEM((Z, HD, LANES), f32),
            pltpu.VMEM((Z + 1, WINDOW, LANES), bf),
            pltpu.VMEM((Z, 8, N), f32),
            pltpu.VMEM((Z, 8, N), f32),
            pltpu.VMEM((Z, N // 2, LANES), bf),
            pltpu.VMEM((Z, N * (CA // LANES - 1), LANES), bf),
            pltpu.VMEM((TP, Z, N // 2, LANES), bf),
            pltpu.VMEM((TP, HOLD, N * (CA // LANES - 1), LANES), bf),
            pltpu.VMEM((Z, 8, N), f32),
            pltpu.VMEM((HOLD, 8, N), f32),
            pltpu.VMEM((N, S * w_out.shape[0]), bf),
            pltpu.VMEM((N, M), f32),
            dma((8,)),
            dma((Z,)), dma((Z, MC)), dma((Z,)), dma((Z, WC)),
            dma((Y - 1, Z)), dma((Y - 1, Z, MC)), dma((Y - 1, Z)), dma((Y - 1, Z, WC)),
            dma((Z,)), dma((Z,)),
            dma((2, Z)), dma((Z, TC)), dma((XH - 1, Z)), dma((XH - 1, Z, TC)),
            dma((XH, Z)), dma((XH, Z, TC)),
            dma((2, Z)), dma((Z, OC)), dma((Y - 1, Z)), dma((Y - 1, Z, OC)),
            dma((Z,)), dma((Z,)), dma((Y - 1, Z)), dma((Y - 1, Z)),
            dma((Z,)), dma((Z,)), dma((Z,)), dma((Z,)), dma((Z,)), dma((Z,)),
            dma((XH - 1, Z)), dma((XH - 1, Z)), dma((XH, Z)), dma((XH, Z)),
            dma((XH - 1, HOLD)), dma((XH - 1, HOLD)), dma((XH, HOLD)), dma((XH, HOLD)),
        ],
        compiler_params=pltpu.CompilerParams(
            collective_id=0, has_side_effects=True, vmem_limit_bytes=60 * 2**20
        ),
    )(tokens, gain, shifts, gates, w_out, *weights, sinks, bias)


def shards(
    tokens,
    norm_gain,
    w_query,
    w_key,
    w_value,
    w_mem_query,
    w_mem_key,
    w_mem_value,
    w_mem_gate,
    w_gates,
    sinks,
    forget_bias,
    forget_shift,
    w_out,
):
    weights = (w_query, w_key, w_value, w_mem_query, w_mem_key, w_mem_value, w_mem_gate)
    mixed, totals = mix(
        tokens,
        norm_gain[None, :],
        forget_shift.T,
        w_gates.transpose(1, 2, 0).reshape(-1, w_gates.shape[0]),
        w_out,
        weights,
        sinks,
        forget_bias,
    )
    return mixed, totals.T


def solution(mesh):
    placed = (
        P(("sp", "tp"), None),
        P(),
        P("sp", "tp"),
        P("sp", "tp"),
        P("sp", "tp"),
        P("sp", "tp"),
        P("sp", "tp"),
        P("sp", "tp"),
        P("sp", "tp"),
        P(),
        P("tp"),
        P("tp"),
        P("sp", "tp"),
        P("sp", "tp"),
    )
    return jax.shard_map(
        shards,
        mesh=mesh,
        in_specs=placed,
        out_specs=(P("sp", "tp"), P("sp", "tp")),
        check_vma=False,
    )
```
